512 devices in a mesh: grp: 2 (over y), fs: 32 (over z, core), tp: 8 (over x).
Axes of the slice: x: 8, y: 2, z: 16, core: 2. Of those that a mesh axis runs over, the one named last changes fastest.
The devices are a block of a 8x8x16 slice.
Arguments:
- tokens: bfloat16 [24576, 2048], P(('grp', 'fs'), 'tp'), parts along dimension 0, may hold values from -6 to 6
- norm_gain: float32 [2048], P('fs'), may hold values from 0.1 to 1.9
- gate_weight: float32 [32, 2048, 1024], P(None, 'fs', 'tp'), may hold values from -0.125 to 0.125
- up_weight: float32 [32, 2048, 1024], P(None, 'fs', 'tp'), may hold values from -0.125 to 0.125
- down_weight: float32 [32, 1024, 2048], P(None, 'fs', 'tp'), may hold values from -0.1875 to 0.1875
- routes: int32 [24576, 2], P(('grp', 'fs')), parts along dimension 0, may hold values from 0 to 31, as said below
- route_weights: float32 [24576, 2], P(('grp', 'fs')), parts along dimension 0, may hold values from 0.2 to 1
Outputs:
- gate_serve: bfloat16 [64, 2048, 1024], P(('grp', 'fs'), None, 'tp'), parts along dimension 0
- up_serve: bfloat16 [64, 2048, 1024], P(('grp', 'fs'), None, 'tp'), parts along dimension 0
- down_serve: bfloat16 [64, 1024, 2048], P(('grp', 'fs'), None, 'tp'), parts along dimension 0
- mixture: bfloat16 [24576, 2048], P(('grp', 'fs'), 'tp'), parts along dimension 0
The draws below stay inside these ranges and needn't reach their ends.
There are 2 independent parts, one for each index of `grp`. The reference program is written for one: setup_inputs(seed, part) draws one part's arguments, and reference() takes and returns one part's arrays. A program takes and returns all parts, laid end to end along the dimension named above; an argument that names none is the same for every part. Nothing has to cross between parts.
Inputs may be any that keep to these rules, and one draw needn't show every extreme that they name: `routes`: each row names two different experts of one group (expert e lies in group e // 8). In each aligned block of 384 rows no expert is named more than 36 times, and every expert of one group is named exactly 36 times.
All inputs are finite; a program needn't handle non-finite values.
Results may differ from the reference program's by a relative error of at most 0.0087.
Values may be sent and summed in bfloat16 or wider, within the bound.
A program may use at most 64 MiB of HBM per device.

```python
import jax
import jax.numpy as jnp
from jax import lax

D = 2048
DE = 1024
NGROUPS = 4
EPG = 8
TOK_DEV = 384
EXPERTS = 32
CAP = 36
TOKENS = 12288


def block_routes(block_key):
    subkeys = jax.random.split(block_key, 6)
    eighth = TOK_DEV // 8
    first_count = jax.random.randint(subkeys[0], (), eighth, 2 * eighth + 1, dtype=jnp.int32)
    second_count = jax.random.randint(subkeys[1], (), eighth, 2 * eighth + 1, dtype=jnp.int32)
    counts = jnp.stack([jnp.int32(3 * eighth), first_count, second_count, jnp.int32(5 * eighth) - first_count - second_count]).astype(jnp.int32)
    starts = (jnp.cumsum(counts) - counts).astype(jnp.int32)
    places = jnp.arange(TOK_DEV, dtype=jnp.int32)
    order_slot = jnp.sum((places[:, None] >= starts[None, 1:]).astype(jnp.int32), axis=1).astype(jnp.int32)
    rank_in_group = places - starts[order_slot]
    group_order = jax.random.permutation(subkeys[2], NGROUPS).astype(jnp.int32)
    group_id = group_order[order_slot]
    member_keys = jax.random.split(subkeys[3], NGROUPS)
    member_perm = jax.vmap(lambda member_key: jax.random.permutation(member_key, EPG))(member_keys).astype(jnp.int32)
    shifts = jax.random.randint(subkeys[4], (NGROUPS, TOK_DEV // EPG + 1), 0, EPG - 1, dtype=jnp.int32)
    lead_member = rank_in_group % EPG
    partner = (rank_in_group + 1 + shifts[order_slot, rank_in_group // EPG]) % EPG
    first_expert = group_id * EPG + member_perm[group_id, lead_member]
    second_expert = group_id * EPG + member_perm[group_id, partner]
    expert_pairs = jnp.stack([first_expert, second_expert], axis=1).astype(jnp.int32)
    shuffle = jax.random.permutation(subkeys[5], TOK_DEV).astype(jnp.int32)
    return jnp.zeros((TOK_DEV, 2), jnp.int32).at[shuffle].set(expert_pairs)


def draw_routes(key, part):
    block_keys = jax.random.split(jax.random.fold_in(key, 17), TOKENS // TOK_DEV)
    return jax.vmap(block_routes)(block_keys).reshape(TOKENS, 2).astype(jnp.int32)


def level_of(rng, shape, shards, smallest, high):
    factor_of = 1.0
    for dim, parts in shards:
        steps = jax.random.uniform(jax.random.fold_in(jax.random.fold_in(rng, 6), dim), (parts,), jnp.float32, smallest / len(shards), high / len(shards))
        factor_of = factor_of * jnp.repeat(jnp.exp(steps), shape[dim] // parts).reshape((-1,) + (1,) * (len(shape) - 1 - dim))
    return factor_of


def normal_values(rng, dims, scale, bound, shards=(), held_as=jnp.bfloat16):
    array = scale * jax.random.normal(rng, dims, jnp.float32)
    if shards:
        array = array * level_of(rng, dims, shards, -0.22, 0.18)
    return jnp.clip(array, -bound, bound).astype(held_as)


def setup_inputs(seed: int = 0, part: int = 0) -> dict:
    splits = jax.random.split(jax.random.key(seed), 8)
    part_keys = jax.random.split(jax.random.fold_in(splits[7], part), 8)
    return {
        "tokens": normal_values(part_keys[0], (TOKENS, D), 1.0, 6.0, ((0, 32), (1, 8))),
        "norm_gain": jnp.clip(1.0 + 0.18 * jax.random.normal(splits[1], (D,), jnp.float32), 0.1, 1.9),
        "gate_weight": normal_values(splits[2], (EXPERTS, D, DE), D ** -0.5, 0.125, ((1, 32), (2, 8)), jnp.float32),
        "up_weight": normal_values(splits[3], (EXPERTS, D, DE), D ** -0.5, 0.125, ((1, 32), (2, 8)), jnp.float32),
        "down_weight": normal_values(splits[4], (EXPERTS, DE, D), DE ** -0.5, 0.1875, ((1, 32), (2, 8)), jnp.float32),
        "routes": draw_routes(jax.random.fold_in(jax.random.fold_in(splits[7], part), 71), part),
        "route_weights": jnp.clip(0.2 + 0.8 * jax.random.uniform(part_keys[6], (TOKENS, 2), jnp.float32) ** level_of(part_keys[6], (TOKENS, 2), ((0, 32),), -0.2, 0.2), 0.2, 1.0),
    }


epsilon = 1e-06

def normalize(rows):
    values = rows.astype(jnp.float32)
    scale = lax.rsqrt(lax.optimization_barrier(jnp.mean(values * values, axis=-1, keepdims=True)) + epsilon)
    return (values * scale).astype(jnp.bfloat16)

def reference(tokens, norm_gain, gate_weight, up_weight, down_weight, routes, route_weights):
    gate_serve = (norm_gain[None, :, None] * gate_weight).astype(jnp.bfloat16)
    up_serve = (norm_gain[None, :, None] * up_weight).astype(jnp.bfloat16)
    down_serve = down_weight.astype(jnp.bfloat16)
    normed = normalize(tokens)
    blocks = TOKENS // TOK_DEV
    span = blocks * CAP
    flat_routes = routes.reshape(blocks, TOK_DEV * 2)
    expert_ids = jnp.arange(EXPERTS, dtype=jnp.int32)
    onehot = (flat_routes[:, :, None] == expert_ids[None, None, :]).astype(jnp.int32)
    position = lax.optimization_barrier(jnp.sum((jnp.cumsum(onehot, axis=1) - 1) * onehot, axis=2)).astype(jnp.int32)
    block_ids = jnp.arange(blocks, dtype=jnp.int32)[:, None]
    destination = (flat_routes * span + block_ids * CAP + position).astype(jnp.int32)
    token_ids = block_ids * TOK_DEV + (jnp.arange(TOK_DEV * 2, dtype=jnp.int32) // 2)[None, :]
    table = jnp.full((EXPERTS * span,), TOKENS, jnp.int32)
    table = table.at[destination.reshape(-1)].set(token_ids.reshape(-1).astype(jnp.int32))
    padded = jnp.concatenate([normed, jnp.zeros((1, D), jnp.bfloat16)], axis=0)

    def expert_rows(operands):
        index_rows, gate_matrix, up_matrix, down_matrix = operands
        rows = padded[index_rows]
        gate_part = jnp.dot(rows, gate_matrix, preferred_element_type=jnp.float32)
        up_part = jnp.dot(rows, up_matrix, preferred_element_type=jnp.float32)
        hidden = (jax.nn.silu(gate_part) * up_part).astype(jnp.bfloat16)
        return jnp.dot(hidden, down_matrix, preferred_element_type=jnp.float32).astype(jnp.bfloat16)
    outputs = lax.map(expert_rows, (table.reshape(EXPERTS, span), gate_serve, up_serve, down_serve))
    picked = outputs.reshape(EXPERTS * span, D)[destination.reshape(TOKENS, 2)]
    mixture = lax.optimization_barrier(jnp.sum(route_weights[:, :, None] * picked.astype(jnp.float32), axis=1)).astype(jnp.bfloat16)
    return (gate_serve, up_serve, down_serve, mixture)
```

```python
import functools

import jax
import jax.numpy as jnp
from jax import lax
from jax.experimental import pallas as pl
from jax.experimental.pallas import tpu as pltpu
from jax.sharding import Mesh
from jax.sharding import PartitionSpec as P

CAP = 36
FS = ("fs_0", "fs_1")
GRP_FS = ("grp", "fs_0", "fs_1")
MESH = pl.DeviceIdType.MESH
EPSILON = 1e-06
CHUNKS = 4


def ring_order(n):
    order = [0]
    for d in range(1, n // 2 + 1):
        order.append(d)
        if len(order) < n:
            order.append(n - d)
    return order


def kernel(
    sizes,
    gate_ref,
    up_ref,
    down_ref,
    outb_ref,
    gate_out,
    up_out,
    down_out,
    ret_ref,
    swap,
    comb,
    x_buf,
    h_buf,
    o_buf,
    gate_v,
    up_v,
    down_v,
    swap_sems,
    tok_s,
    tok_r,
    gu_s,
    gu_r,
    dn_s,
    dn_r,
    ygu_s,
    ygu_r,
    ydn_s,
    ydn_r,
    xs,
    xr,
    hs,
    hr,
    ret_s,
    ret_r,
    fin_s,
    fin_r,
    out_sem,
):
    n_z, n_x, n_grp = sizes
    order = ring_order(n_z)
    per = n_z // CHUNKS
    slot, width = x_buf.shape[2], x_buf.shape[3]
    g_half = gate_v.shape[1] // 2
    d_half = down_v.shape[1] // 2
    grp = lax.axis_index("grp")
    z = lax.axis_index("fs_0")
    core = lax.axis_index("fs_1")
    x = lax.axis_index("tp")
    me = z * 2 + core
    half = lax.rem(grp, 2)
    y_peer = {"grp": grp + 1 - 2 * half}
    other_core = {"fs_1": 1 - core}
    right = {"tp": lax.rem(x + 1, n_x)}
    left = {"tp": lax.rem(x + n_x - 1, n_x)}
    sends = []

    def ahead(pos):
        return lax.rem(z + order[pos], n_z)

    def behind(pos):
        return lax.rem(z + n_z - order[pos], n_z)

    def remote(src, dst, send_sem, recv_sem, device):
        return pltpu.make_async_remote_copy(
            src_ref=src, dst_ref=dst, send_sem=send_sem, recv_sem=recv_sem, device_id=device, device_id_type=MESH
        )

    def send(*args):
        copy = remote(*args)
        copy.start()
        sends.append(copy)
        return copy

    barrier = pltpu.get_barrier_semaphore()
    peers = [y_peer, other_core, right, left]
    for pos in range(1, n_z):
        for c in range(2):
            peers.append({"fs_0": ahead(pos), "fs_1": c})
    for device in peers:
        pl.semaphore_signal(barrier, inc=1, device_id=device, device_id_type=MESH)
    pl.semaphore_wait(barrier, len(peers))

    first = send(outb_ref.at[1], swap, swap_sems.at[0], swap_sems.at[1], other_core)
    first.wait_recv()
    comb[...] = outb_ref[0] + swap[...]
    x_buf[0, 0] = outb_ref[0, 0] + swap[0]

    for pos in range(1, n_z):
        send(comb.at[pos], x_buf.at[0, pos], tok_s.at[pos], tok_r.at[pos], {"fs_0": ahead(pos)})

    g_rows = pl.ds(pl.multiple_of(half * g_half, g_half), g_half)
    d_rows = pl.ds(pl.multiple_of(half * d_half, d_half), d_half)
    gate_v[me] = gate_ref[me]
    up_v[me] = up_ref[me]
    down_v[me] = down_ref[me]
    mate = z * 2 + 1 - core
    send(gate_ref.at[mate], gate_v.at[me], gu_s.at[0, 0, 0], gu_r.at[0, 0, 0], other_core)
    send(up_ref.at[mate], up_v.at[me], gu_s.at[0, 0, 1], gu_r.at[0, 0, 1], other_core)
    send(down_ref.at[mate], down_v.at[me], dn_s.at[0, 0], dn_r.at[0, 0], other_core)
    for pos in range(1, n_z):
        for c in range(2):
            cc = lax.rem(core + c, 2)
            e = ahead(pos) * 2 + cc
            device = {"fs_0": ahead(pos), "fs_1": cc}
            send(gate_ref.at[e, g_rows], gate_v.at[me, g_rows], gu_s.at[pos, c, 0], gu_r.at[pos, c, 0], device)
            send(up_ref.at[e, g_rows], up_v.at[me, g_rows], gu_s.at[pos, c, 1], gu_r.at[pos, c, 1], device)
    for pos in range(1, n_z):
        for c in range(2):
            cc = lax.rem(core + c, 2)
            e = ahead(pos) * 2 + cc
            device = {"fs_0": ahead(pos), "fs_1": cc}
            send(down_ref.at[e, d_rows], down_v.at[me, d_rows], dn_s.at[pos, c], dn_r.at[pos, c], device)

    def got(ref, sem):
        pltpu.make_async_copy(ref, ref, sem).wait()

    def wait_tokens(k):
        for pos in range(k * per, (k + 1) * per):
            if pos:
                got(x_buf.at[0, pos], tok_r.at[pos])

    def hop(buf, k, h, s_sems, r_sems):
        whole = pl.ds(k * per, per)
        first_half, second_half = pl.ds(k * per, per // 2), pl.ds(k * per + per // 2, per // 2)
        last = n_x // 2
        if h > 1:
            arrived(buf, k, h - 1, r_sems)
        rows = first_half if h == last else whole
        send(buf.at[h - 1, rows], buf.at[h, rows], s_sems.at[k, h - 1, 0], r_sems.at[k, h - 1, 0], right)
        rows = second_half if h == last else whole
        send(buf.at[(n_x - h + 1) % n_x, rows], buf.at[n_x - h, rows], s_sems.at[k, h - 1, 1], r_sems.at[k, h - 1, 1], left)

    def arrived(buf, k, h, r_sems):
        last = n_x // 2
        whole = pl.ds(k * per, per)
        first_half, second_half = pl.ds(k * per, per // 2), pl.ds(k * per + per // 2, per // 2)
        got(buf.at[h, first_half if h == last else whole], r_sems.at[k, h - 1, 0])
        got(buf.at[n_x - h, second_half if h == last else whole], r_sems.at[k, h - 1, 1])

    def forward_gu(k):
        for pos in range(max(1, k * per), (k + 1) * per):
            for c in range(2):
                cc = lax.rem(core + c, 2)
                s = behind(pos) * 2 + cc
                got(gate_v.at[s, g_rows], gu_r.at[pos, c, 0])
                got(up_v.at[s, g_rows], gu_r.at[pos, c, 1])
            pair = pl.ds(behind(pos) * 2, 2)
            send(gate_v.at[pair, g_rows], gate_v.at[pair, g_rows], ygu_s.at[pos, 0], ygu_r.at[pos, 0], y_peer)
            send(up_v.at[pair, g_rows], up_v.at[pair, g_rows], ygu_s.at[pos, 1], ygu_r.at[pos, 1], y_peer)

    def forward_dn(k):
        for pos in range(max(1, k * per), (k + 1) * per):
            for c in range(2):
                cc = lax.rem(core + c, 2)
                got(down_v.at[behind(pos) * 2 + cc, d_rows], dn_r.at[pos, c])
            pair = pl.ds(behind(pos) * 2, 2)
            send(down_v.at[pair, d_rows], down_v.at[pair, d_rows], ydn_s.at[pos], ydn_r.at[pos], y_peer)

    def hop_x(k, h):
        if h == 1:
            wait_tokens(k)
        hop(x_buf, k, h, xs, xr)

    hop_x(0, 1)
    hop_x(1, 1)
    hop_x(0, 2)
    hop_x(1, 2)
    hop_x(0, 3)
    hop_x(1, 3)
    hop_x(2, 1)
    hop_x(0, 4)
    hop_x(1, 4)
    hop_x(3, 1)
    hop_x(2, 2)
    hop_x(3, 2)
    forward_gu(0)
    hop_x(2, 3)
    forward_gu(1)
    hop_x(3, 3)
    forward_gu(2)
    hop_x(2, 4)
    hop_x(3, 4)
    forward_gu(3)

    o_g_rows = pl.ds(pl.multiple_of((1 - half) * g_half, g_half), g_half)
    o_d_rows = pl.ds(pl.multiple_of((1 - half) * d_half, d_half), d_half)
    got(gate_v.at[mate], gu_r.at[0, 0, 0])
    got(up_v.at[mate], gu_r.at[0, 0, 1])
    for pos in range(1, n_z):
        pair = pl.ds(behind(pos) * 2, 2)
        got(gate_v.at[pair, o_g_rows], ygu_r.at[pos, 0])
        got(up_v.at[pair, o_g_rows], ygu_r.at[pos, 1])
    outs = [
        pltpu.make_async_copy(gate_v, gate_out, out_sem.at[0]),
        pltpu.make_async_copy(up_v, up_out, out_sem.at[1]),
        pltpu.make_async_copy(down_v, down_out, out_sem.at[2]),
    ]
    outs[0].start()
    outs[1].start()

    f_src = 2 * n_z // n_x
    rows = per * slot

    def expert_hidden(k):
        for h in ((4,) if k < 2 else (4,)):
            arrived(x_buf, k, h, xr)
        total = jnp.zeros((rows, 2 * gate_v.shape[2]), jnp.float32)
        square = jnp.zeros((rows, width), jnp.float32)
        for s in range(n_x):
            t = lax.rem(x + n_x - s, n_x)
            block = x_buf[s, k * per : (k + 1) * per].reshape(rows, width)
            src = pl.ds(t * f_src, f_src)
            w = jnp.concatenate(
                [gate_v[src].reshape(width, gate_v.shape[2]), up_v[src].reshape(width, up_v.shape[2])], axis=1
            )
            total = total + jnp.dot(block, w, preferred_element_type=jnp.float32)
            wide = block.astype(jnp.float32)
            square = square + wide * wide
        scale = lax.rsqrt(jnp.sum(square, axis=1, keepdims=True) * (1.0 / (n_x * width)) + EPSILON)
        n_h = gate_v.shape[2]
        g = total[:, :n_h] * scale
        u = total[:, n_h:] * scale
        hidden = (g / (1.0 + jnp.exp(-g))) * u
        h_buf[0, k * per : (k + 1) * per] = hidden.astype(jnp.bfloat16).reshape(per, slot, n_h)

    def hop_h(k, h):
        hop(h_buf, k, h, hs, hr)

    def expert_out(k):
        arrived(h_buf, k, 4, hr)
        n_h = h_buf.shape[3]
        total = jnp.zeros((rows, width), jnp.float32)
        for s in range(n_x):
            t = lax.rem(x + n_x - s, n_x)
            w = down_v[pl.ds(t * f_src, f_src)].reshape(n_h, width)
            block = h_buf[s, k * per : (k + 1) * per].reshape(rows, n_h)
            total = total + jnp.dot(block, w, preferred_element_type=jnp.float32)
        o_buf[k * per : (k + 1) * per] = total.astype(jnp.bfloat16).reshape(per, slot, width)

    def send_out(k):
        for pos in reversed(range(k * per, (k + 1) * per)):
            if pos:
                send(o_buf.at[pos], ret_ref.at[0, pos], ret_s.at[pos], ret_r.at[pos], {"fs_0": behind(pos)})
            else:
                ret_ref[0, 0] = o_buf[0]

    expert_hidden(3)
    hop_h(3, 1)
    expert_hidden(2)
    hop_h(2, 1)
    hop_h(3, 2)
    expert_hidden(1)
    hop_h(2, 2)
    hop_h(3, 3)
    hop_h(1, 1)
    hop_h(2, 3)
    expert_hidden(0)
    hop_h(3, 4)
    hop_h(2, 4)
    hop_h(0, 1)
    hop_h(1, 2)
    for k in range(CHUNKS):
        forward_dn(k)
    hop_h(0, 2)
    hop_h(1, 3)
    got(down_v.at[mate], dn_r.at[0, 0])
    for pos in range(1, n_z):
        got(down_v.at[pl.ds(behind(pos) * 2, 2), o_d_rows], ydn_r.at[pos])
    outs[2].start()
    expert_out(3)
    send_out(3)
    hop_h(0, 3)
    hop_h(1, 4)
    expert_out(2)
    send_out(2)
    hop_h(0, 4)
    expert_out(1)
    send_out(1)
    expert_out(0)
    send_out(0)

    for k in reversed(range(CHUNKS)):
        part = pl.ds(k * per, per)
        for pos in range(k * per, (k + 1) * per):
            if pos:
                got(ret_ref.at[0, pos], ret_r.at[pos])
        send(ret_ref.at[0, part], ret_ref.at[1, part], fin_s.at[k], fin_r.at[k], other_core)
    for k in reversed(range(CHUNKS)):
        got(ret_ref.at[1, pl.ds(k * per, per)], fin_r.at[k])
    for copy in outs:
        copy.wait()
    for copy in sends:
        copy.wait_send()


def exchange_and_apply(gate_low, up_low, down_low, outb, sizes):
    n_z, n_x, n_grp = sizes
    bf16 = jnp.bfloat16
    _, _, slot, width = outb.shape
    n_h = gate_low.shape[2]
    dma = pltpu.SemaphoreType.DMA
    hops = n_x // 2
    vmem = pl.BlockSpec(memory_space=pltpu.VMEM)
    hbm = pl.BlockSpec(memory_space=pl.ANY)
    return pl.pallas_call(
        functools.partial(kernel, sizes),
        out_shape=(
            jax.ShapeDtypeStruct(gate_low.shape, bf16),
            jax.ShapeDtypeStruct(up_low.shape, bf16),
            jax.ShapeDtypeStruct(down_low.shape, bf16),
            jax.ShapeDtypeStruct(outb.shape, bf16),
        ),
        in_specs=[vmem] * 4,
        out_specs=(hbm, hbm, hbm, vmem),
        scratch_shapes=[
            pltpu.VMEM(outb.shape[1:], bf16),
            pltpu.VMEM(outb.shape[1:], bf16),
            pltpu.VMEM((n_x, n_z, slot, width), bf16),
            pltpu.VMEM((n_x, n_z, slot, n_h), bf16),
            pltpu.VMEM(outb.shape[1:], bf16),
            pltpu.VMEM(gate_low.shape, bf16),
            pltpu.VMEM(up_low.shape, bf16),
            pltpu.VMEM(down_low.shape, bf16),
            dma((2,)),
            dma((n_z,)),
            dma((n_z,)),
            dma((n_z, 2, 2)),
            dma((n_z, 2, 2)),
            dma((n_z, 2)),
            dma((n_z, 2)),
            dma((n_z, 2)),
            dma((n_z, 2)),
            dma((n_z,)),
            dma((n_z,)),
            dma((CHUNKS, hops, 2)),
            dma((CHUNKS, hops, 2)),
            dma((CHUNKS, hops, 2)),
            dma((CHUNKS, hops, 2)),
            dma((n_z,)),
            dma((n_z,)),
            dma((CHUNKS,)),
            dma((CHUNKS,)),
            dma((3,)),
        ],
        compiler_params=pltpu.CompilerParams(
            collective_id=0, has_side_effects=True, vmem_limit_bytes=40 * 1024 * 1024
        ),
        name="exchange_and_apply",
    )(gate_low, up_low, down_low, outb)


def shards(tokens, norm_gain, gate_weight, up_weight, down_weight, routes, route_weights):
    experts = gate_weight.shape[0]
    n_z = lax.axis_size("fs_0")
    n_x = lax.axis_size("tp")
    n_grp = lax.axis_size("grp")
    tok_rows, width = tokens.shape
    gate_low = (norm_gain[None, :, None] * gate_weight).astype(jnp.bfloat16)
    up_low = (norm_gain[None, :, None] * up_weight).astype(jnp.bfloat16)
    down_low = down_weight.astype(jnp.bfloat16)

    flat_routes = routes.reshape(-1)
    expert_ids = lax.iota(jnp.int32, experts)
    onehot = (flat_routes[:, None] == expert_ids[None, :]).astype(jnp.int32)
    position = jnp.sum((jnp.cumsum(onehot, axis=0) - 1) * onehot, axis=1)
    order = ring_order(n_z)
    distance = lax.rem(flat_routes // 2 - lax.axis_index("fs_0") + n_z, n_z)
    pos = jnp.where(distance == 0, 0, jnp.where(distance <= n_z // 2, 2 * distance - 1, 2 * (n_z - distance)))
    crossed = jnp.abs(lax.rem(flat_routes, 2) - lax.axis_index("fs_1"))
    slots = 2 * CAP
    slot_index = (crossed * (n_z * slots + CAP) + pos * slots + position).reshape(tok_rows, 2)
    slot_ids = lax.iota(jnp.int32, 2 * n_z * slots)
    select = jnp.any(slot_ids[:, None, None] == slot_index[None, :, :], axis=2).astype(jnp.bfloat16)
    outbound = jnp.dot(select, tokens, preferred_element_type=jnp.float32).astype(jnp.bfloat16)
    outbound = outbound.reshape(2, n_z, slots, width)
    gate_serve, up_serve, down_serve, back = exchange_and_apply(
        gate_low, up_low, down_low, outbound, (n_z, n_x, n_grp)
    )
    picked = back.reshape(2 * n_z * slots, width)[slot_index]
    mixture = jnp.sum(route_weights[:, :, None] * picked.astype(jnp.float32), axis=1).astype(
        jnp.bfloat16
    )
    return (
        gate_serve.reshape(1, -1, gate_serve.shape[2]),
        up_serve.reshape(1, -1, up_serve.shape[2]),
        down_serve.reshape(1, -1, down_serve.shape[2]),
        mixture,
    )


def solution(mesh):
    split = Mesh(
        mesh.devices.reshape(mesh.shape["grp"], mesh.shape["fs"] // 2, 2, mesh.shape["tp"]),
        ("grp", "fs_0", "fs_1", "tp"),
    )
    placed = (
        P(GRP_FS, "tp"),
        P(FS),
        P(None, FS, "tp"),
        P(None, FS, "tp"),
        P(None, FS, "tp"),
        P(GRP_FS, None),
        P(GRP_FS, None),
    )
    return jax.shard_map(
        shards,
        mesh=split,
        in_specs=placed,
        out_specs=(
            P(GRP_FS, None, "tp"),
            P(GRP_FS, None, "tp"),
            P(GRP_FS, None, "tp"),
            P(GRP_FS, "tp"),
        ),
        check_vma=False,
    )
```

```python
import functools

import jax
import jax.numpy as jnp
from jax import lax
from jax.experimental import pallas as pl
from jax.experimental.pallas import tpu as pltpu
from jax.sharding import Mesh
from jax.sharding import PartitionSpec as P

CAP = 36
FS = ("fs_0", "fs_1")
GRP_FS = ("grp", "fs_0", "fs_1")
MESH = pl.DeviceIdType.MESH
EPSILON = 1e-06
CHUNKS = 4


def ring_order(n):
    order = [0]
    for d in range(1, n // 2 + 1):
        order.append(d)
        if len(order) < n:
            order.append(n - d)
    return order


def kernel(
    sizes,
    tok_ref,
    route_ref,
    mix_ref,
    gain_ref,
    gate_in,
    up_in,
    down_in,
    gate_out,
    up_out,
    down_out,
    mixture_ref,
    wide_v,
    wide_d,
    gate_ref,
    up_ref,
    down_ref,
    place_v,
    pick_hi,
    pick_lo,
    outb_ref,
    ret_ref,
    swap,
    comb,
    x_buf,
    h_buf,
    o_buf,
    gate_v,
    up_v,
    down_v,
    swap_sems,
    tok_s,
    tok_r,
    gu_s,
    gu_r,
    dn_s,
    dn_r,
    ygu_s,
    ygu_r,
    ydn_s,
    ydn_r,
    xs,
    xr,
    hs,
    hr,
    ret_s,
    ret_r,
    fin_s,
    fin_r,
    out_sem,
    in_sem,
):
    n_z, n_x, n_grp = sizes
    order = ring_order(n_z)
    per = n_z // CHUNKS
    slot, width = x_buf.shape[2], x_buf.shape[3]
    g_half = gate_v.shape[1] // 2
    d_half = down_v.shape[1] // 2
    grp = lax.axis_index("grp")
    z = lax.axis_index("fs_0")
    core = lax.axis_index("fs_1")
    x = lax.axis_index("tp")
    me = z * 2 + core
    half = lax.rem(grp, 2)
    y_peer = {"grp": grp + 1 - 2 * half}
    other_core = {"fs_1": 1 - core}
    right = {"tp": lax.rem(x + 1, n_x)}
    left = {"tp": lax.rem(x + n_x - 1, n_x)}
    sends = []

    def ahead(pos):
        return lax.rem(z + order[pos], n_z)

    def behind(pos):
        return lax.rem(z + n_z - order[pos], n_z)

    def remote(src, dst, send_sem, recv_sem, device):
        return pltpu.make_async_remote_copy(
            src_ref=src, dst_ref=dst, send_sem=send_sem, recv_sem=recv_sem, device_id=device, device_id_type=MESH
        )

    def send(*args):
        copy = remote(*args)
        copy.start()
        sends.append(copy)
        return copy

    barrier = pltpu.get_barrier_semaphore()
    peers = [y_peer, other_core, right, left]
    for pos in range(1, n_z):
        for c in range(2):
            peers.append({"fs_0": ahead(pos), "fs_1": c})
    for device in peers:
        pl.semaphore_signal(barrier, inc=1, device_id=device, device_id_type=MESH)

    loads = [
        pltpu.make_async_copy(gate_in, wide_v.at[0], in_sem.at[0]),
        pltpu.make_async_copy(up_in, wide_v.at[1], in_sem.at[1]),
        pltpu.make_async_copy(down_in, wide_d, in_sem.at[2]),
    ]
    for copy in loads:
        copy.start()

    f32, bf16 = jnp.float32, jnp.bfloat16
    n_tok = tok_ref.shape[0]
    experts = 2 * n_z
    expert_ids = lax.broadcasted_iota(jnp.int32, (experts, n_tok), 0)
    names = [jnp.where(expert_ids == route_ref[k : k + 1, :], 1.0, 0.0) for k in range(2)]
    named = names[0] + names[1]
    before = lax.broadcasted_iota(jnp.int32, (n_tok, n_tok), 0) < lax.broadcasted_iota(jnp.int32, (n_tok, n_tok), 1)
    before = jnp.where(before, 1.0, 0.0).astype(bf16)
    place = jnp.dot(named.astype(bf16), before, preferred_element_type=f32)
    place_v[...] = jnp.where(named > 0.5, place, -1.0 - slot)

    def dispatch(j, crossed):
        distance = jnp.where(lax.rem(j, 2) == 1, (j + 1) // 2, n_z - j // 2)
        e = lax.rem(z + distance, n_z) * 2 + jnp.where(crossed == 1, 1 - core, core)
        slot_ids = lax.broadcasted_iota(jnp.int32, (slot, n_tok), 0).astype(f32) - CAP * crossed
        pick = jnp.where(slot_ids == place_v[pl.ds(e, 1), :], 1.0, 0.0).astype(bf16)
        outb_ref[crossed, j] = jnp.dot(pick, tok_ref[...], preferred_element_type=f32).astype(bf16)

    def dispatch_both(j, carry):
        dispatch(j, 1)
        dispatch(j, 0)
        return carry

    lax.fori_loop(0, n_z, dispatch_both, 0)
    pl.semaphore_wait(barrier, len(peers))

    first = send(outb_ref.at[1], swap, swap_sems.at[0], swap_sems.at[1], other_core)

    n_gain = gain_ref.shape[1]
    eye = lax.broadcasted_iota(jnp.int32, (n_gain, n_gain), 0) == lax.broadcasted_iota(jnp.int32, (n_gain, n_gain), 1)
    gain = jnp.sum(jnp.where(eye, gain_ref[...], 0.0), axis=1, keepdims=True)
    for copy in loads:
        copy.wait()

    def cast(e, carry):
        gate_ref[e] = (gain * wide_v[0, e]).astype(bf16)
        up_ref[e] = (gain * wide_v[1, e]).astype(bf16)
        down_ref[e] = wide_d[e].astype(bf16)
        return carry

    lax.fori_loop(0, experts, cast, 0)

    first.wait_recv()
    comb[...] = outb_ref[0] + swap[...]
    x_buf[0, 0] = outb_ref[0, 0] + swap[0]
    gate_v[me] = gate_ref[me]
    up_v[me] = up_ref[me]
    down_v[me] = down_ref[me]

    for pos in range(1, n_z):
        send(comb.at[pos], x_buf.at[0, pos], tok_s.at[pos], tok_r.at[pos], {"fs_0": ahead(pos)})

    g_rows = pl.ds(pl.multiple_of(half * g_half, g_half), g_half)
    d_rows = pl.ds(pl.multiple_of(half * d_half, d_half), d_half)
    mate = z * 2 + 1 - core
    send(gate_ref.at[mate], gate_v.at[me], gu_s.at[0, 0, 0], gu_r.at[0, 0, 0], other_core)
    send(up_ref.at[mate], up_v.at[me], gu_s.at[0, 0, 1], gu_r.at[0, 0, 1], other_core)
    send(down_ref.at[mate], down_v.at[me], dn_s.at[0, 0], dn_r.at[0, 0], other_core)
    for pos in range(1, n_z):
        for c in range(2):
            cc = lax.rem(core + c, 2)
            e = ahead(pos) * 2 + cc
            device = {"fs_0": ahead(pos), "fs_1": cc}
            send(gate_ref.at[e, g_rows], gate_v.at[me, g_rows], gu_s.at[pos, c, 0], gu_r.at[pos, c, 0], device)
            send(up_ref.at[e, g_rows], up_v.at[me, g_rows], gu_s.at[pos, c, 1], gu_r.at[pos, c, 1], device)
    for pos in range(1, n_z):
        for c in range(2):
            cc = lax.rem(core + c, 2)
            e = ahead(pos) * 2 + cc
            device = {"fs_0": ahead(pos), "fs_1": cc}
            send(down_ref.at[e, d_rows], down_v.at[me, d_rows], dn_s.at[pos, c], dn_r.at[pos, c], device)

    def got(ref, sem):
        pltpu.make_async_copy(ref, ref, sem).wait()

    def wait_tokens(k):
        for pos in range(k * per, (k + 1) * per):
            if pos:
                got(x_buf.at[0, pos], tok_r.at[pos])

    def hop(buf, k, h, s_sems, r_sems):
        whole = pl.ds(k * per, per)
        first_half, second_half = pl.ds(k * per, per // 2), pl.ds(k * per + per // 2, per // 2)
        last = n_x // 2
        if h > 1:
            arrived(buf, k, h - 1, r_sems)
        rows = first_half if h == last else whole
        send(buf.at[h - 1, rows], buf.at[h, rows], s_sems.at[k, h - 1, 0], r_sems.at[k, h - 1, 0], right)
        rows = second_half if h == last else whole
        send(buf.at[(n_x - h + 1) % n_x, rows], buf.at[n_x - h, rows], s_sems.at[k, h - 1, 1], r_sems.at[k, h - 1, 1], left)

    def arrived(buf, k, h, r_sems):
        last = n_x // 2
        whole = pl.ds(k * per, per)
        first_half, second_half = pl.ds(k * per, per // 2), pl.ds(k * per + per // 2, per // 2)
        got(buf.at[h, first_half if h == last else whole], r_sems.at[k, h - 1, 0])
        got(buf.at[n_x - h, second_half if h == last else whole], r_sems.at[k, h - 1, 1])

    def forward_gu(k):
        for pos in range(max(1, k * per), (k + 1) * per):
            for c in range(2):
                cc = lax.rem(core + c, 2)
                s = behind(pos) * 2 + cc
                got(gate_v.at[s, g_rows], gu_r.at[pos, c, 0])
                got(up_v.at[s, g_rows], gu_r.at[pos, c, 1])
            pair = pl.ds(behind(pos) * 2, 2)
            send(gate_v.at[pair, g_rows], gate_v.at[pair, g_rows], ygu_s.at[pos, 0], ygu_r.at[pos, 0], y_peer)
            send(up_v.at[pair, g_rows], up_v.at[pair, g_rows], ygu_s.at[pos, 1], ygu_r.at[pos, 1], y_peer)

    def forward_dn(k):
        for pos in range(max(1, k * per), (k + 1) * per):
            for c in range(2):
                cc = lax.rem(core + c, 2)
                got(down_v.at[behind(pos) * 2 + cc, d_rows], dn_r.at[pos, c])
            pair = pl.ds(behind(pos) * 2, 2)
            send(down_v.at[pair, d_rows], down_v.at[pair, d_rows], ydn_s.at[pos], ydn_r.at[pos], y_peer)

    def build_picks():
        chosen = []
        for k in range(2):
            e = route_ref[k : k + 1, :]
            far = lax.rem(e // 2 - z + n_z, n_z)
            pos = jnp.where(far == 0, 0, jnp.where(far <= n_z // 2, 2 * far - 1, 2 * (n_z - far)))
            crossed = jnp.where(lax.rem(e, 2) == core, 0, 1)
            inside = jnp.sum(names[k] * place, axis=0, keepdims=True)
            chosen.append((crossed * (n_z * slot + CAP) + pos * slot).astype(f32) + inside)
        chosen += [mix_ref[0:1, :], mix_ref[1:2, :]]
        table = jnp.concatenate(chosen + [jnp.zeros((128 - len(chosen), n_tok), f32)], axis=0).T
        step = per * slot
        for c in range(2 * CHUNKS):
            ids = (lax.broadcasted_iota(jnp.int32, (n_tok, step), 1) + c * step).astype(f32)
            w = jnp.where(ids == table[:, 0:1], table[:, 2:3], 0.0) + jnp.where(ids == table[:, 1:2], table[:, 3:4], 0.0)
            hi = w.astype(bf16)
            pick_hi[c] = hi
            pick_lo[c] = (w - hi.astype(f32)).astype(bf16)

    def hop_x(k, h):
        if h == 1:
            wait_tokens(k)
        hop(x_buf, k, h, xs, xr)

    hop_x(0, 1)
    hop_x(1, 1)
    hop_x(0, 2)
    hop_x(1, 2)
    hop_x(0, 3)
    hop_x(1, 3)
    hop_x(2, 1)
    hop_x(0, 4)
    hop_x(1, 4)
    hop_x(2, 2)
    build_picks()
    hop_x(2, 3)
    hop_x(3, 1)
    hop_x(2, 4)
    hop_x(3, 2)
    forward_gu(0)
    forward_gu(1)
    hop_x(3, 3)
    forward_gu(2)
    hop_x(3, 4)
    forward_gu(3)

    o_g_rows = pl.ds(pl.multiple_of((1 - half) * g_half, g_half), g_half)
    o_d_rows = pl.ds(pl.multiple_of((1 - half) * d_half, d_half), d_half)
    got(gate_v.at[mate], gu_r.at[0, 0, 0])
    got(up_v.at[mate], gu_r.at[0, 0, 1])
    for pos in range(1, n_z):
        pair = pl.ds(behind(pos) * 2, 2)
        got(gate_v.at[pair, o_g_rows], ygu_r.at[pos, 0])
        got(up_v.at[pair, o_g_rows], ygu_r.at[pos, 1])
    outs = [
        pltpu.make_async_copy(gate_v, gate_out, out_sem.at[0]),
        pltpu.make_async_copy(up_v, up_out, out_sem.at[1]),
        pltpu.make_async_copy(down_v, down_out, out_sem.at[2]),
    ]
    outs[0].start()
    outs[1].start()

    f_src = 2 * n_z // n_x
    rows = per * slot

    def expert_hidden(k):
        arrived(x_buf, k, n_x // 2, xr)
        total = jnp.zeros((rows, 2 * gate_v.shape[2]), jnp.float32)
        square = jnp.zeros((rows, width), jnp.float32)
        for s in range(n_x):
            t = lax.rem(x + n_x - s, n_x)
            block = x_buf[s, k * per : (k + 1) * per].reshape(rows, width)
            src = pl.ds(t * f_src, f_src)
            w = jnp.concatenate(
                [gate_v[src].reshape(width, gate_v.shape[2]), up_v[src].reshape(width, up_v.shape[2])], axis=1
            )
            total = total + jnp.dot(block, w, preferred_element_type=jnp.float32)
            wide = block.astype(jnp.float32)
            square = square + wide * wide
        scale = lax.rsqrt(jnp.sum(square, axis=1, keepdims=True) * (1.0 / (n_x * width)) + EPSILON)
        n_h = gate_v.shape[2]
        g = total[:, :n_h] * scale
        u = total[:, n_h:] * scale
        hidden = (g / (1.0 + jnp.exp(-g))) * u
        h_buf[0, k * per : (k + 1) * per] = hidden.astype(jnp.bfloat16).reshape(per, slot, n_h)

    def hop_h(k, h):
        hop(h_buf, k, h, hs, hr)

    def expert_out(k):
        arrived(h_buf, k, n_x // 2, hr)
        n_h = h_buf.shape[3]
        total = jnp.zeros((rows, width), jnp.float32)
        for s in range(n_x):
            t = lax.rem(x + n_x - s, n_x)
            w = down_v[pl.ds(t * f_src, f_src)].reshape(n_h, width)
            block = h_buf[s, k * per : (k + 1) * per].reshape(rows, n_h)
            total = total + jnp.dot(block, w, preferred_element_type=jnp.float32)
        o_buf[k * per : (k + 1) * per] = total.astype(jnp.bfloat16).reshape(per, slot, width)

    def send_out(k):
        for pos in reversed(range(k * per, (k + 1) * per)):
            if pos:
                send(o_buf.at[pos], ret_ref.at[0, pos], ret_s.at[pos], ret_r.at[pos], {"fs_0": behind(pos)})
            else:
                ret_ref[0, 0] = o_buf[0]

    expert_hidden(3)
    hop_h(3, 1)
    expert_hidden(2)
    hop_h(2, 1)
    hop_h(3, 2)
    expert_hidden(1)
    hop_h(2, 2)
    hop_h(3, 3)
    hop_h(1, 1)
    hop_h(2, 3)
    hop_h(3, 4)
    expert_hidden(0)
    hop_h(0, 1)
    hop_h(2, 4)
    hop_h(1, 2)
    for k in range(CHUNKS):
        forward_dn(k)
    hop_h(0, 2)
    got(down_v.at[mate], dn_r.at[0, 0])
    for pos in range(1, n_z):
        got(down_v.at[pl.ds(behind(pos) * 2, 2), o_d_rows], ydn_r.at[pos])
    outs[2].start()
    expert_out(3)
    send_out(3)
    hop_h(1, 3)
    hop_h(0, 3)
    expert_out(2)
    send_out(2)
    hop_h(1, 4)
    hop_h(0, 4)
    expert_out(1)
    send_out(1)
    expert_out(0)
    send_out(0)

    def mixed(c, k):
        data = ret_ref[c, k * per : (k + 1) * per].reshape(rows, width)
        part = jnp.dot(pick_hi[c * CHUNKS + k], data, preferred_element_type=f32)
        return part + jnp.dot(pick_lo[c * CHUNKS + k], data, preferred_element_type=f32)

    total = jnp.zeros((n_tok, width), f32)
    backs = (3, 2, 1, 0)
    for n, k in enumerate(backs):
        for pos in range(k * per, (k + 1) * per):
            if pos:
                got(ret_ref.at[0, pos], ret_r.at[pos])
        part = pl.ds(k * per, per)
        send(ret_ref.at[0, part], ret_ref.at[1, part], fin_s.at[k], fin_r.at[k], other_core)
        total = total + mixed(0, k)
        if n:
            got(ret_ref.at[1, pl.ds(backs[n - 1] * per, per)], fin_r.at[backs[n - 1]])
            total = total + mixed(1, backs[n - 1])
    got(ret_ref.at[1, pl.ds(backs[-1] * per, per)], fin_r.at[backs[-1]])
    total = total + mixed(1, backs[-1])
    mixture_ref[...] = total.astype(bf16)
    for copy in outs:
        copy.wait()
    for copy in sends:
        copy.wait_send()


def exchange_and_apply(tokens, routes, mix, gain, gate, up, down, sizes):
    n_z, n_x, n_grp = sizes
    f32, bf16 = jnp.float32, jnp.bfloat16
    n_tok, width = tokens.shape
    slot = 2 * CAP
    n_h = gate.shape[2]
    experts = gate.shape[0]
    dma = pltpu.SemaphoreType.DMA
    hops = n_x // 2
    vmem = pl.BlockSpec(memory_space=pltpu.VMEM)
    hbm = pl.BlockSpec(memory_space=pl.ANY)
    picks = (2 * CHUNKS, n_tok, n_z // CHUNKS * slot)
    return pl.pallas_call(
        functools.partial(kernel, sizes),
        out_shape=(
            jax.ShapeDtypeStruct(gate.shape, bf16),
            jax.ShapeDtypeStruct(up.shape, bf16),
            jax.ShapeDtypeStruct(down.shape, bf16),
            jax.ShapeDtypeStruct(tokens.shape, bf16),
        ),
        in_specs=[vmem] * 4 + [hbm] * 3,
        out_specs=(hbm, hbm, hbm, vmem),
        scratch_shapes=[
            pltpu.VMEM((2,) + gate.shape, f32),
            pltpu.VMEM(down.shape, f32),
            pltpu.VMEM(gate.shape, bf16),
            pltpu.VMEM(up.shape, bf16),
            pltpu.VMEM(down.shape, bf16),
            pltpu.VMEM((experts, n_tok), f32),
            pltpu.VMEM(picks, bf16),
            pltpu.VMEM(picks, bf16),
            pltpu.VMEM((2, n_z, slot, width), bf16),
            pltpu.VMEM((2, n_z, slot, width), bf16),
            pltpu.VMEM((n_z, slot, width), bf16),
            pltpu.VMEM((n_z, slot, width), bf16),
            pltpu.VMEM((n_x, n_z, slot, width), bf16),
            pltpu.VMEM((n_x, n_z, slot, n_h), bf16),
            pltpu.VMEM((n_z, slot, width), bf16),
            pltpu.VMEM(gate.shape, bf16),
            pltpu.VMEM(up.shape, bf16),
            pltpu.VMEM(down.shape, bf16),
            dma((2,)),
            dma((n_z,)),
            dma((n_z,)),
            dma((n_z, 2, 2)),
            dma((n_z, 2, 2)),
            dma((n_z, 2)),
            dma((n_z, 2)),
            dma((n_z, 2)),
            dma((n_z, 2)),
            dma((n_z,)),
            dma((n_z,)),
            dma((CHUNKS, hops, 2)),
            dma((CHUNKS, hops, 2)),
            dma((CHUNKS, hops, 2)),
            dma((CHUNKS, hops, 2)),
            dma((n_z,)),
            dma((n_z,)),
            dma((CHUNKS,)),
            dma((CHUNKS,)),
            dma((3,)),
            dma((3,)),
        ],
        compiler_params=pltpu.CompilerParams(
            collective_id=0, has_side_effects=True, vmem_limit_bytes=40 * 1024 * 1024
        ),
        name="exchange_and_apply",
    )(tokens, routes, mix, gain, gate, up, down)


def shards(tokens, norm_gain, gate_weight, up_weight, down_weight, routes, route_weights):
    sizes = (lax.axis_size("fs_0"), lax.axis_size("tp"), lax.axis_size("grp"))
    gate_serve, up_serve, down_serve, mixture = exchange_and_apply(
        tokens, routes.T, route_weights.T, norm_gain[None, :], gate_weight, up_weight, down_weight, sizes
    )
    return (
        gate_serve.reshape(1, -1, gate_serve.shape[2]),
        up_serve.reshape(1, -1, up_serve.shape[2]),
        down_serve.reshape(1, -1, down_serve.shape[2]),
        mixture,
    )


def solution(mesh):
    split = Mesh(
        mesh.devices.reshape(mesh.shape["grp"], mesh.shape["fs"] // 2, 2, mesh.shape["tp"]),
        ("grp", "fs_0", "fs_1", "tp"),
    )
    placed = (
        P(GRP_FS, "tp"),
        P(FS),
        P(None, FS, "tp"),
        P(None, FS, "tp"),
        P(None, FS, "tp"),
        P(GRP_FS, None),
        P(GRP_FS, None),
    )
    return jax.shard_map(
        shards,
        mesh=split,
        in_specs=placed,
        out_specs=(
            P(GRP_FS, None, "tp"),
            P(GRP_FS, None, "tp"),
            P(GRP_FS, None, "tp"),
            P(GRP_FS, "tp"),
        ),
        check_vma=False,
    )
```

```python
import functools

import jax
import jax.numpy as jnp
from jax import lax
from jax.experimental import pallas as pl
from jax.experimental.pallas import tpu as pltpu
from jax.sharding import Mesh
from jax.sharding import PartitionSpec as P

CAP = 36
FS = ("fs_0", "fs_1")
GRP_FS = ("grp", "fs_0", "fs_1")
MESH = pl.DeviceIdType.MESH
EPSILON = 1e-06
CHUNKS = 8


def ring_order(n):
    order = [0]
    for d in range(1, n // 2 + 1):
        order.append(d)
        if len(order) < n:
            order.append(n - d)
    return order


def kernel(
    sizes,
    tok_ref,
    route_ref,
    mix_ref,
    gain_ref,
    gate_in,
    up_in,
    down_in,
    gate_out,
    up_out,
    down_out,
    mixture_ref,
    wide_v,
    wide_d,
    gate_ref,
    up_ref,
    down_ref,
    place_v,
    pick_hi,
    pick_lo,
    outb_ref,
    ret_ref,
    swap,
    comb,
    x_buf,
    h_buf,
    o_buf,
    gate_v,
    up_v,
    down_v,
    swap_sems,
    tok_s,
    tok_r,
    gu_s,
    gu_r,
    dn_s,
    dn_r,
    ygu_s,
    ygu_r,
    ydn_s,
    ydn_r,
    xs,
    xr,
    hs,
    hr,
    ret_s,
    ret_r,
    fin_s,
    fin_r,
    out_sem,
    in_sem,
    stage_x,
    stage_gu,
    stage_dn,
    stage_s,
    stage_r,
):
    n_z, n_x, n_grp = sizes
    order = ring_order(n_z)
    per = n_z // CHUNKS
    slot, width = x_buf.shape[2], x_buf.shape[3]
    g_half = gate_v.shape[1] // 2
    d_half = down_v.shape[1] // 2
    grp = lax.axis_index("grp")
    z = lax.axis_index("fs_0")
    core = lax.axis_index("fs_1")
    x = lax.axis_index("tp")
    me = z * 2 + core
    half = lax.rem(grp, 2)
    y_peer = {"grp": grp + 1 - 2 * half}
    other_core = {"fs_1": 1 - core}
    right = {"tp": lax.rem(x + 1, n_x)}
    left = {"tp": lax.rem(x + n_x - 1, n_x)}
    sends, late_sends = [], []

    def ahead(pos):
        return lax.rem(z + order[pos], n_z)

    def behind(pos):
        return lax.rem(z + n_z - order[pos], n_z)

    def remote(src, dst, send_sem, recv_sem, device):
        return pltpu.make_async_remote_copy(
            src_ref=src, dst_ref=dst, send_sem=send_sem, recv_sem=recv_sem, device_id=device, device_id_type=MESH
        )

    def send(*args):
        copy = remote(*args)
        copy.start()
        sends.append(copy)
        return copy

    barrier = pltpu.get_barrier_semaphore()
    peers = [y_peer, other_core, right, left]
    for pos in range(1, n_z):
        for c in range(2):
            peers.append({"fs_0": ahead(pos), "fs_1": c})
    for device in peers:
        pl.semaphore_signal(barrier, inc=1, device_id=device, device_id_type=MESH)

    loads = [
        pltpu.make_async_copy(gate_in, wide_v.at[0], in_sem.at[0]),
        pltpu.make_async_copy(up_in, wide_v.at[1], in_sem.at[1]),
        pltpu.make_async_copy(down_in, wide_d, in_sem.at[2]),
    ]
    for copy in loads:
        copy.start()

    f32, bf16 = jnp.float32, jnp.bfloat16
    n_tok = tok_ref.shape[0]
    experts = 2 * n_z
    expert_ids = lax.broadcasted_iota(jnp.int32, (experts, n_tok), 0)
    names = [jnp.where(expert_ids == route_ref[k : k + 1, :], 1.0, 0.0) for k in range(2)]
    named = names[0] + names[1]
    before = lax.broadcasted_iota(jnp.int32, (n_tok, n_tok), 0) < lax.broadcasted_iota(jnp.int32, (n_tok, n_tok), 1)
    before = jnp.where(before, 1.0, 0.0).astype(bf16)
    place = jnp.dot(named.astype(bf16), before, preferred_element_type=f32)
    place_v[...] = jnp.where(named > 0.5, place, -1.0 - slot)

    def dispatch(j, crossed):
        distance = jnp.where(lax.rem(j, 2) == 1, (j + 1) // 2, n_z - j // 2)
        e = lax.rem(z + distance, n_z) * 2 + jnp.where(crossed == 1, 1 - core, core)
        slot_ids = lax.broadcasted_iota(jnp.int32, (slot, n_tok), 0).astype(f32) - CAP * crossed
        pick = jnp.where(slot_ids == place_v[pl.ds(e, 1), :], 1.0, 0.0).astype(bf16)
        outb_ref[crossed, j] = jnp.dot(pick, tok_ref[...], preferred_element_type=f32).astype(bf16)

    def dispatch_both(j, carry):
        dispatch(j, 1)
        dispatch(j, 0)
        return carry

    lax.fori_loop(0, n_z, dispatch_both, 0)
    pl.semaphore_wait(barrier, len(peers))

    first = send(outb_ref.at[1], swap, swap_sems.at[0], swap_sems.at[1], other_core)

    n_gain = gain_ref.shape[1]
    eye = lax.broadcasted_iota(jnp.int32, (n_gain, n_gain), 0) == lax.broadcasted_iota(jnp.int32, (n_gain, n_gain), 1)
    gain = jnp.sum(jnp.where(eye, gain_ref[...], 0.0), axis=1, keepdims=True)
    for copy in loads:
        copy.wait()

    def cast(e, carry):
        gate_ref[e] = (gain * wide_v[0, e]).astype(bf16)
        up_ref[e] = (gain * wide_v[1, e]).astype(bf16)
        down_ref[e] = wide_d[e].astype(bf16)
        return carry

    lax.fori_loop(0, experts, cast, 0)

    first.wait_recv()
    comb[...] = outb_ref[0] + swap[...]
    x_buf[0, 0] = outb_ref[0, 0] + swap[0]
    gate_v[me] = gate_ref[me]
    up_v[me] = up_ref[me]
    down_v[me] = down_ref[me]

    opposite = n_z - 1
    leg = {"fs_0": lax.rem(z + n_z - n_z // 4, n_z)}
    origin = lax.rem(z + n_z // 4, n_z) * 2 + 1
    relays = core == 1

    def leg_dest(c):
        return {"fs_0": lax.rem(z + n_z - n_z // 4, n_z), "fs_1": c}

    def first_leg(n, src, stage):
        remote(src, stage, stage_s.at[n, 0], stage_r.at[n], leg).start()

    def second_leg(n, stage, dst, recv_sem, device):
        got(stage, stage_r.at[n])
        remote(stage, dst, stage_s.at[n, 1], recv_sem, device).start()

    def got(ref, sem):
        pltpu.make_async_copy(ref, ref, sem).wait()

    @pl.when(relays)
    def _():
        first_leg(0, comb.at[opposite], stage_x.at[0])

    for pos in range(1, n_z - 1):
        send(comb.at[pos], x_buf.at[0, pos], tok_s.at[pos], tok_r.at[pos], {"fs_0": ahead(pos)})

    @pl.when(jnp.logical_not(relays))
    def _():
        remote(
            comb.at[opposite], x_buf.at[0, opposite], tok_s.at[opposite], tok_r.at[opposite], {"fs_0": ahead(opposite)}
        ).start()

    def relay_tokens():
        @pl.when(relays)
        def _():
            second_leg(0, stage_x.at[0], x_buf.at[0, opposite], tok_r.at[opposite], leg)

    g_rows = pl.ds(pl.multiple_of(half * g_half, g_half), g_half)
    d_rows = pl.ds(pl.multiple_of(half * d_half, d_half), d_half)
    mate = z * 2 + 1 - core
    send(gate_ref.at[mate], gate_v.at[me], gu_s.at[0, 0, 0], gu_r.at[0, 0, 0], other_core)
    send(up_ref.at[mate], up_v.at[me], gu_s.at[0, 0, 1], gu_r.at[0, 0, 1], other_core)
    send(down_ref.at[mate], down_v.at[me], dn_s.at[0, 0], dn_r.at[0, 0], other_core)
    def gate_up_copies(pos, c):
        cc = lax.rem(core + c, 2)
        e = ahead(pos) * 2 + cc
        device = {"fs_0": ahead(pos), "fs_1": cc}
        return (
            remote(gate_ref.at[e, g_rows], gate_v.at[me, g_rows], gu_s.at[pos, c, 0], gu_r.at[pos, c, 0], device),
            remote(up_ref.at[e, g_rows], up_v.at[me, g_rows], gu_s.at[pos, c, 1], gu_r.at[pos, c, 1], device),
        )

    def down_copies(pos, c):
        cc = lax.rem(core + c, 2)
        e = ahead(pos) * 2 + cc
        device = {"fs_0": ahead(pos), "fs_1": cc}
        return (remote(down_ref.at[e, d_rows], down_v.at[me, d_rows], dn_s.at[pos, c], dn_r.at[pos, c], device),)

    def send_weights(copies_of):
        for pos in range(1, n_z - 1):
            for c in range(2):
                for copy in copies_of(pos, c):
                    copy.start()
                    sends.append(copy)

        @pl.when(jnp.logical_not(relays))
        def _():
            for c in range(2):
                for copy in copies_of(opposite, c):
                    copy.start()

    def send_gate_up():
        @pl.when(relays)
        def _():
            for c in range(2):
                e = ahead(opposite) * 2 + c
                first_leg(1 + 2 * c, gate_ref.at[e, g_rows], stage_gu.at[c, 0])
                first_leg(2 + 2 * c, up_ref.at[e, g_rows], stage_gu.at[c, 1])

        send_weights(gate_up_copies)

    def relay_gate_up():
        @pl.when(relays)
        def _():
            for c in range(2):
                n = 1 - c
                second_leg(
                    1 + 2 * c, stage_gu.at[c, 0], gate_v.at[origin, g_rows], gu_r.at[opposite, n, 0], leg_dest(c)
                )
                second_leg(2 + 2 * c, stage_gu.at[c, 1], up_v.at[origin, g_rows], gu_r.at[opposite, n, 1], leg_dest(c))

    def send_down():
        @pl.when(relays)
        def _():
            for c in range(2):
                first_leg(5 + c, down_ref.at[ahead(opposite) * 2 + c, d_rows], stage_dn.at[c])

        send_weights(down_copies)

    def relay_down():
        @pl.when(relays)
        def _():
            for c in range(2):
                second_leg(5 + c, stage_dn.at[c], down_v.at[origin, d_rows], dn_r.at[opposite, 1 - c], leg_dest(c))

    def relay_back():
        @pl.when(relays)
        def _():
            second_leg(7, stage_x.at[1], ret_ref.at[0, opposite], ret_r.at[opposite], leg)

    def wait_tokens(k):
        for pos in range(k * per, (k + 1) * per):
            if pos:
                got(x_buf.at[0, pos], tok_r.at[pos])

    def hop(buf, k, h, s_sems, r_sems):
        whole = pl.ds(k * per, per)
        first_half, second_half = pl.ds(k * per, per // 2), pl.ds(k * per + per // 2, per // 2)
        last = n_x // 2
        if h > 1:
            arrived(buf, k, h - 1, r_sems)
        rows = first_half if h == last else whole
        send(buf.at[h - 1, rows], buf.at[h, rows], s_sems.at[k, h - 1, 0], r_sems.at[k, h - 1, 0], right)
        rows = second_half if h == last else whole
        send(buf.at[(n_x - h + 1) % n_x, rows], buf.at[n_x - h, rows], s_sems.at[k, h - 1, 1], r_sems.at[k, h - 1, 1], left)

    def arrived(buf, k, h, r_sems):
        last = n_x // 2
        whole = pl.ds(k * per, per)
        first_half, second_half = pl.ds(k * per, per // 2), pl.ds(k * per + per // 2, per // 2)
        got(buf.at[h, first_half if h == last else whole], r_sems.at[k, h - 1, 0])
        got(buf.at[n_x - h, second_half if h == last else whole], r_sems.at[k, h - 1, 1])

    def forward_gu(k):
        for pos in range(max(1, k * per), (k + 1) * per):
            for c in range(2):
                cc = lax.rem(core + c, 2)
                s = behind(pos) * 2 + cc
                got(gate_v.at[s, g_rows], gu_r.at[pos, c, 0])
                got(up_v.at[s, g_rows], gu_r.at[pos, c, 1])
            pair = pl.ds(behind(pos) * 2, 2)
            send(gate_v.at[pair, g_rows], gate_v.at[pair, g_rows], ygu_s.at[pos, 0], ygu_r.at[pos, 0], y_peer)
            send(up_v.at[pair, g_rows], up_v.at[pair, g_rows], ygu_s.at[pos, 1], ygu_r.at[pos, 1], y_peer)

    def forward_dn(k):
        for pos in range(max(1, k * per), (k + 1) * per):
            for c in range(2):
                cc = lax.rem(core + c, 2)
                got(down_v.at[behind(pos) * 2 + cc, d_rows], dn_r.at[pos, c])
            pair = pl.ds(behind(pos) * 2, 2)
            send(down_v.at[pair, d_rows], down_v.at[pair, d_rows], ydn_s.at[pos], ydn_r.at[pos], y_peer)

    def build_picks():
        chosen = []
        for k in range(2):
            e = route_ref[k : k + 1, :]
            far = lax.rem(e // 2 - z + n_z, n_z)
            pos = jnp.where(far == 0, 0, jnp.where(far <= n_z // 2, 2 * far - 1, 2 * (n_z - far)))
            crossed = jnp.where(lax.rem(e, 2) == core, 0, 1)
            inside = jnp.sum(names[k] * place, axis=0, keepdims=True)
            chosen.append((crossed * (n_z * slot + CAP) + pos * slot).astype(f32) + inside)
        chosen += [mix_ref[0:1, :], mix_ref[1:2, :]]
        table = jnp.concatenate(chosen + [jnp.zeros((128 - len(chosen), n_tok), f32)], axis=0).T
        step = per * slot
        for c in range(2 * CHUNKS):
            ids = (lax.broadcasted_iota(jnp.int32, (n_tok, step), 1) + c * step).astype(f32)
            w = jnp.where(ids == table[:, 0:1], table[:, 2:3], 0.0) + jnp.where(ids == table[:, 1:2], table[:, 3:4], 0.0)
            hi = w.astype(bf16)
            pick_hi[c] = hi
            pick_lo[c] = (w - hi.astype(f32)).astype(bf16)

    def hop_x(k, h):
        if h == 1:
            wait_tokens(k)
        hop(x_buf, k, h, xs, xr)

    top = n_x // 2
    begins = (0, 0, 1, 2, 2, 3, 4, 5)
    gate_up_rounds = {6: (0, 1, 2), 7: (3, 4, 5), 8: (6, 7)}
    for r in range(begins[-1] + top):
        for k in range(CHUNKS):
            if 0 <= r - begins[k] < top:
                hop_x(k, r - begins[k] + 1)
        if r == 1:
            relay_tokens()
            send_gate_up()
        if r == 2:
            build_picks()
        if r == 5:
            relay_gate_up()
            send_down()
        for k in gate_up_rounds.get(r, ()):
            forward_gu(k)

    relay_down()

    o_g_rows = pl.ds(pl.multiple_of((1 - half) * g_half, g_half), g_half)
    o_d_rows = pl.ds(pl.multiple_of((1 - half) * d_half, d_half), d_half)
    got(gate_v.at[mate], gu_r.at[0, 0, 0])
    got(up_v.at[mate], gu_r.at[0, 0, 1])
    for pos in range(1, n_z):
        pair = pl.ds(behind(pos) * 2, 2)
        got(gate_v.at[pair, o_g_rows], ygu_r.at[pos, 0])
        got(up_v.at[pair, o_g_rows], ygu_r.at[pos, 1])
    outs = [
        pltpu.make_async_copy(gate_v, gate_out, out_sem.at[0]),
        pltpu.make_async_copy(up_v, up_out, out_sem.at[1]),
        pltpu.make_async_copy(down_v, down_out, out_sem.at[2]),
    ]
    outs[0].start()
    outs[1].start()

    def wait_down():
        got(down_v.at[mate], dn_r.at[0, 0])
        for pos in range(1, n_z):
            got(down_v.at[pl.ds(behind(pos) * 2, 2), o_d_rows], ydn_r.at[pos])
        outs[2].start()

    f_src = 2 * n_z // n_x
    rows = per * slot

    def expert_hidden(k):
        arrived(x_buf, k, n_x // 2, xr)
        total = jnp.zeros((rows, 2 * gate_v.shape[2]), jnp.float32)
        square = jnp.zeros((rows, width), jnp.float32)
        for s in range(n_x):
            t = lax.rem(x + n_x - s, n_x)
            block = x_buf[s, k * per : (k + 1) * per].reshape(rows, width)
            src = pl.ds(t * f_src, f_src)
            w = jnp.concatenate(
                [gate_v[src].reshape(width, gate_v.shape[2]), up_v[src].reshape(width, up_v.shape[2])], axis=1
            )
            total = total + jnp.dot(block, w, preferred_element_type=jnp.float32)
            wide = block.astype(jnp.float32)
            square = square + wide * wide
        scale = lax.rsqrt(jnp.sum(square, axis=1, keepdims=True) * (1.0 / (n_x * width)) + EPSILON)
        n_h = gate_v.shape[2]
        g = total[:, :n_h] * scale
        u = total[:, n_h:] * scale
        hidden = (g / (1.0 + jnp.exp(-g))) * u
        h_buf[0, k * per : (k + 1) * per] = hidden.astype(jnp.bfloat16).reshape(per, slot, n_h)

    def hop_h(k, h):
        hop(h_buf, k, h, hs, hr)

    def expert_out(k):
        arrived(h_buf, k, n_x // 2, hr)
        n_h = h_buf.shape[3]
        total = jnp.zeros((rows, width), jnp.float32)
        for s in range(n_x):
            t = lax.rem(x + n_x - s, n_x)
            w = down_v[pl.ds(t * f_src, f_src)].reshape(n_h, width)
            block = h_buf[s, k * per : (k + 1) * per].reshape(rows, n_h)
            total = total + jnp.dot(block, w, preferred_element_type=jnp.float32)
        o_buf[k * per : (k + 1) * per] = total.astype(jnp.bfloat16).reshape(per, slot, width)

    def send_out(k):
        for pos in reversed(range(k * per, (k + 1) * per)):
            if pos:
                copy = remote(o_buf.at[pos], ret_ref.at[0, pos], ret_s.at[pos], ret_r.at[pos], {"fs_0": behind(pos)})
                if pos < opposite:
                    copy.start()
                    late_sends.append(copy)
                    continue

                @pl.when(relays)
                def _():
                    first_leg(7, o_buf.at[pos], stage_x.at[1])

                @pl.when(jnp.logical_not(relays))
                def _():
                    copy.start()
            else:
                ret_ref[0, 0] = o_buf[0]

    near, far = tuple(range(CHUNKS // 2 - 1, -1, -1)), tuple(range(CHUNKS - 1, CHUNKS // 2 - 1, -1))

    def hops(chunks, h):
        for k in chunks:
            if h == 1:
                expert_hidden(k)
            hop_h(k, h)

    def finish(chunks):
        for k in chunks:
            expert_out(k)
            send_out(k)

    hops(far, 1)
    for k in range(0, 5):
        forward_dn(k)
    hops(far, 2)
    forward_dn(5)
    hops(near, 1)
    hops(far, 3)
    forward_dn(6)
    hops(near, 2)
    forward_dn(7)
    hops(far, 4)
    wait_down()
    finish(far[:2])
    hops(near, 3)
    finish(far[2:])
    relay_back()
    hops(near, 4)
    finish(near)
    for copy in sends:
        copy.wait_send()
    sends.clear()
    outs[0].wait()
    outs[1].wait()
    outs[2].wait()

    def mixed(c, k):
        data = ret_ref[c, k * per : (k + 1) * per].reshape(rows, width)
        part = jnp.dot(pick_hi[c * CHUNKS + k], data, preferred_element_type=f32)
        return part + jnp.dot(pick_lo[c * CHUNKS + k], data, preferred_element_type=f32)

    total = jnp.zeros((n_tok, width), f32)
    backs = tuple(reversed(range(CHUNKS)))
    for n, k in enumerate(backs):
        for pos in range(k * per, (k + 1) * per):
            if pos:
                got(ret_ref.at[0, pos], ret_r.at[pos])
        part = pl.ds(k * per, per)
        copy = remote(ret_ref.at[0, part], ret_ref.at[1, part], fin_s.at[k], fin_r.at[k], other_core)
        copy.start()
        late_sends.append(copy)
        total = total + mixed(0, k)
        if n:
            got(ret_ref.at[1, pl.ds(backs[n - 1] * per, per)], fin_r.at[backs[n - 1]])
            total = total + mixed(1, backs[n - 1])
    got(ret_ref.at[1, pl.ds(backs[-1] * per, per)], fin_r.at[backs[-1]])
    total = total + mixed(1, backs[-1])
    mixture_ref[...] = total.astype(bf16)
    for copy in late_sends:
        copy.wait_send()

    @pl.when(relays)
    def _():
        for n in range(2):
            got(stage_x.at[0], stage_s.at[0, n])
            got(stage_x.at[1], stage_s.at[7, n])
            for c in range(2):
                got(stage_gu.at[c, 0], stage_s.at[1 + 2 * c, n])
                got(stage_gu.at[c, 1], stage_s.at[2 + 2 * c, n])
                got(stage_dn.at[c], stage_s.at[5 + c, n])

    @pl.when(jnp.logical_not(relays))
    def _():
        got(comb.at[opposite], tok_s.at[opposite])
        got(o_buf.at[opposite], ret_s.at[opposite])
        for c in range(2):
            got(stage_gu.at[c, 0], gu_s.at[opposite, c, 0])
            got(stage_gu.at[c, 1], gu_s.at[opposite, c, 1])
            got(stage_dn.at[c], dn_s.at[opposite, c])


def exchange_and_apply(tokens, routes, mix, gain, gate, up, down, sizes):
    n_z, n_x, n_grp = sizes
    f32, bf16 = jnp.float32, jnp.bfloat16
    n_tok, width = tokens.shape
    slot = 2 * CAP
    n_h = gate.shape[2]
    experts = gate.shape[0]
    dma = pltpu.SemaphoreType.DMA
    hops = n_x // 2
    vmem = pl.BlockSpec(memory_space=pltpu.VMEM)
    hbm = pl.BlockSpec(memory_space=pl.ANY)
    picks = (2 * CHUNKS, n_tok, n_z // CHUNKS * slot)
    return pl.pallas_call(
        functools.partial(kernel, sizes),
        out_shape=(
            jax.ShapeDtypeStruct(gate.shape, bf16),
            jax.ShapeDtypeStruct(up.shape, bf16),
            jax.ShapeDtypeStruct(down.shape, bf16),
            jax.ShapeDtypeStruct(tokens.shape, bf16),
        ),
        in_specs=[vmem] * 4 + [hbm] * 3,
        out_specs=(hbm, hbm, hbm, vmem),
        scratch_shapes=[
            pltpu.VMEM((2,) + gate.shape, f32),
            pltpu.VMEM(down.shape, f32),
            pltpu.VMEM(gate.shape, bf16),
            pltpu.VMEM(up.shape, bf16),
            pltpu.VMEM(down.shape, bf16),
            pltpu.VMEM((experts, n_tok), f32),
            pltpu.VMEM(picks, bf16),
            pltpu.VMEM(picks, bf16),
            pltpu.VMEM((2, n_z, slot, width), bf16),
            pltpu.VMEM((2, n_z, slot, width), bf16),
            pltpu.VMEM((n_z, slot, width), bf16),
            pltpu.VMEM((n_z, slot, width), bf16),
            pltpu.VMEM((n_x, n_z, slot, width), bf16),
            pltpu.VMEM((n_x, n_z, slot, n_h), bf16),
            pltpu.VMEM((n_z, slot, width), bf16),
            pltpu.VMEM(gate.shape, bf16),
            pltpu.VMEM(up.shape, bf16),
            pltpu.VMEM(down.shape, bf16),
            dma((2,)),
            dma((n_z,)),
            dma((n_z,)),
            dma((n_z, 2, 2)),
            dma((n_z, 2, 2)),
            dma((n_z, 2)),
            dma((n_z, 2)),
            dma((n_z, 2)),
            dma((n_z, 2)),
            dma((n_z,)),
            dma((n_z,)),
            dma((CHUNKS, hops, 2)),
            dma((CHUNKS, hops, 2)),
            dma((CHUNKS, hops, 2)),
            dma((CHUNKS, hops, 2)),
            dma((n_z,)),
            dma((n_z,)),
            dma((CHUNKS,)),
            dma((CHUNKS,)),
            dma((3,)),
            dma((3,)),
            pltpu.VMEM((2, slot, width), bf16),
            pltpu.VMEM((2, 2, gate.shape[1] // 2, n_h), bf16),
            pltpu.VMEM((2, down.shape[1] // 2, width), bf16),
            dma((8, 2)),
            dma((8,)),
        ],
        compiler_params=pltpu.CompilerParams(
            collective_id=0, has_side_effects=True, vmem_limit_bytes=67043328
        ),
        name="exchange_and_apply",
    )(tokens, routes, mix, gain, gate, up, down)


def shards(tokens, norm_gain, gate_weight, up_weight, down_weight, routes, route_weights):
    sizes = (lax.axis_size("fs_0"), lax.axis_size("tp"), lax.axis_size("grp"))
    gate_serve, up_serve, down_serve, mixture = exchange_and_apply(
        tokens, routes.T, route_weights.T, norm_gain[None, :], gate_weight, up_weight, down_weight, sizes
    )
    return (
        gate_serve.reshape(1, -1, gate_serve.shape[2]),
        up_serve.reshape(1, -1, up_serve.shape[2]),
        down_serve.reshape(1, -1, down_serve.shape[2]),
        mixture,
    )


def solution(mesh):
    split = Mesh(
        mesh.devices.reshape(mesh.shape["grp"], mesh.shape["fs"] // 2, 2, mesh.shape["tp"]),
        ("grp", "fs_0", "fs_1", "tp"),
    )
    placed = (
        P(GRP_FS, "tp"),
        P(FS),
        P(None, FS, "tp"),
        P(None, FS, "tp"),
        P(None, FS, "tp"),
        P(GRP_FS, None),
        P(GRP_FS, None),
    )
    return jax.shard_map(
        shards,
        mesh=split,
        in_specs=placed,
        out_specs=(
            P(GRP_FS, None, "tp"),
            P(GRP_FS, None, "tp"),
            P(GRP_FS, None, "tp"),
            P(GRP_FS, "tp"),
        ),
        check_vma=False,
    )
```

```python
import functools

import jax
import jax.numpy as jnp
from jax import lax
from jax.experimental import pallas as pl
from jax.experimental.pallas import tpu as pltpu
from jax.sharding import Mesh
from jax.sharding import PartitionSpec as P

CAP = 36
FS = ("fs_0", "fs_1")
GRP_FS = ("grp", "fs_0", "fs_1")
MESH = pl.DeviceIdType.MESH
EPSILON = 1e-06
CHUNKS = 8


def ring_order(n):
    order = [0]
    for d in range(1, n // 2 + 1):
        order.append(d)
        if len(order) < n:
            order.append(n - d)
    return order


def kernel(
    sizes,
    tok_ref,
    route_ref,
    mix_ref,
    gain_ref,
    gate_in,
    up_in,
    down_in,
    gate_out,
    up_out,
    down_out,
    mixture_ref,
    wide_v,
    wide_d,
    gate_ref,
    up_ref,
    down_ref,
    place_v,
    pick_hi,
    pick_lo,
    outb_ref,
    ret_ref,
    swap,
    comb,
    x_buf,
    h_buf,
    o_buf,
    gate_v,
    up_v,
    down_v,
    swap_sems,
    tok_s,
    tok_r,
    gu_s,
    gu_r,
    dn_s,
    dn_r,
    ygu_s,
    ygu_r,
    ydn_s,
    ydn_r,
    xs,
    xr,
    hs,
    hr,
    ret_s,
    ret_r,
    fin_s,
    fin_r,
    out_sem,
    in_sem,
    stage_x,
    stage_gu,
    stage_dn,
    stage_s,
    stage_r,
):
    n_z, n_x, n_grp = sizes
    order = ring_order(n_z)
    per = n_z // CHUNKS
    slot, width = x_buf.shape[2], x_buf.shape[3]
    g_half = gate_v.shape[1] // 2
    d_half = down_v.shape[1] // 2
    grp = lax.axis_index("grp")
    z = lax.axis_index("fs_0")
    core = lax.axis_index("fs_1")
    x = lax.axis_index("tp")
    me = z * 2 + core
    half = lax.rem(grp, 2)
    y_peer = {"grp": grp + 1 - 2 * half}
    other_core = {"fs_1": 1 - core}
    right = {"tp": lax.rem(x + 1, n_x)}
    left = {"tp": lax.rem(x + n_x - 1, n_x)}

    def ahead(pos):
        return lax.rem(z + order[pos], n_z)

    def behind(pos):
        return lax.rem(z + n_z - order[pos], n_z)

    def remote(src, dst, send_sem, recv_sem, device):
        return pltpu.make_async_remote_copy(
            src_ref=src, dst_ref=dst, send_sem=send_sem, recv_sem=recv_sem, device_id=device, device_id_type=MESH
        )

    def send(*args):
        copy = remote(*args)
        copy.start()
        return copy

    barrier = pltpu.get_barrier_semaphore()
    peers = [y_peer, other_core, right, left]
    for pos in range(1, n_z):
        for c in range(2):
            peers.append({"fs_0": ahead(pos), "fs_1": c})
    for device in peers:
        pl.semaphore_signal(barrier, inc=1, device_id=device, device_id_type=MESH)

    loads = [
        pltpu.make_async_copy(gate_in, wide_v.at[0], in_sem.at[0]),
        pltpu.make_async_copy(up_in, wide_v.at[1], in_sem.at[1]),
        pltpu.make_async_copy(down_in, wide_d, in_sem.at[2]),
    ]
    for copy in loads:
        copy.start()

    f32, bf16 = jnp.float32, jnp.bfloat16
    n_tok = tok_ref.shape[0]
    experts = 2 * n_z
    expert_ids = lax.broadcasted_iota(jnp.int32, (experts, n_tok), 0)
    names = [jnp.where(expert_ids == route_ref[k : k + 1, :], 1.0, 0.0) for k in range(2)]
    named = names[0] + names[1]
    before = lax.broadcasted_iota(jnp.int32, (n_tok, n_tok), 0) < lax.broadcasted_iota(jnp.int32, (n_tok, n_tok), 1)
    before = jnp.where(before, 1.0, 0.0).astype(bf16)
    place = jnp.dot(named.astype(bf16), before, preferred_element_type=f32)
    place_v[...] = jnp.where(named > 0.5, place, -1.0 - slot)

    def dispatch(j, crossed):
        distance = jnp.where(lax.rem(j, 2) == 1, (j + 1) // 2, n_z - j // 2)
        e = lax.rem(z + distance, n_z) * 2 + jnp.where(crossed == 1, 1 - core, core)
        slot_ids = lax.broadcasted_iota(jnp.int32, (slot, n_tok), 0).astype(f32) - CAP * crossed
        pick = jnp.where(slot_ids == place_v[pl.ds(e, 1), :], 1.0, 0.0).astype(bf16)
        outb_ref[crossed, j] = jnp.dot(pick, tok_ref[...], preferred_element_type=f32).astype(bf16)

    def dispatch_both(j, carry):
        dispatch(j, 1)
        dispatch(j, 0)
        return carry

    lax.fori_loop(0, n_z, dispatch_both, 0)
    pl.semaphore_wait(barrier, len(peers))

    first = send(outb_ref.at[1], swap, swap_sems.at[0], swap_sems.at[1], other_core)

    n_gain = gain_ref.shape[1]
    eye = lax.broadcasted_iota(jnp.int32, (n_gain, n_gain), 0) == lax.broadcasted_iota(jnp.int32, (n_gain, n_gain), 1)
    gain = jnp.sum(jnp.where(eye, gain_ref[...], 0.0), axis=1, keepdims=True)
    for copy in loads:
        copy.wait()

    def cast(e, carry):
        gate_ref[e] = (gain * wide_v[0, e]).astype(bf16)
        up_ref[e] = (gain * wide_v[1, e]).astype(bf16)
        down_ref[e] = wide_d[e].astype(bf16)
        return carry

    lax.fori_loop(0, experts, cast, 0)

    first.wait_recv()
    comb[...] = outb_ref[0] + swap[...]
    x_buf[0, 0] = outb_ref[0, 0] + swap[0]
    gate_v[me] = gate_ref[me]
    up_v[me] = up_ref[me]
    down_v[me] = down_ref[me]

    opposite = n_z - 1
    leg = {"fs_0": lax.rem(z + n_z - n_z // 4, n_z)}
    origin = lax.rem(z + n_z // 4, n_z) * 2 + 1
    relays = core == 1

    def leg_dest(c):
        return {"fs_0": lax.rem(z + n_z - n_z // 4, n_z), "fs_1": c}

    def first_leg(n, src, stage):
        remote(src, stage, stage_s.at[n, 0], stage_r.at[n], leg).start()

    def second_leg(n, stage, dst, recv_sem, device):
        got(stage, stage_r.at[n])
        remote(stage, dst, stage_s.at[n, 1], recv_sem, device).start()

    def got(ref, sem):
        pltpu.make_async_copy(ref, ref, sem).wait()

    @pl.when(relays)
    def _():
        first_leg(0, comb.at[opposite], stage_x.at[0])

    for pos in range(1, n_z - 1):
        send(comb.at[pos], x_buf.at[0, pos], tok_s.at[0], tok_r.at[pos], {"fs_0": ahead(pos)})

    @pl.when(jnp.logical_not(relays))
    def _():
        remote(
            comb.at[opposite], x_buf.at[0, opposite], tok_s.at[0], tok_r.at[opposite], {"fs_0": ahead(opposite)}
        ).start()

    def relay_tokens():
        @pl.when(relays)
        def _():
            second_leg(0, stage_x.at[0], x_buf.at[0, opposite], tok_r.at[opposite], leg)

    g_rows = pl.ds(pl.multiple_of(half * g_half, g_half), g_half)
    d_rows = pl.ds(pl.multiple_of(half * d_half, d_half), d_half)
    mate = z * 2 + 1 - core
    send(gate_ref.at[mate], gate_v.at[me], gu_s.at[0], gu_r.at[0, 0, 0], other_core)
    send(up_ref.at[mate], up_v.at[me], gu_s.at[0], gu_r.at[0, 0, 1], other_core)
    send(down_ref.at[mate], down_v.at[me], dn_s.at[0], dn_r.at[0, 0], other_core)
    def gate_up_copies(pos, c):
        cc = lax.rem(core + c, 2)
        e = ahead(pos) * 2 + cc
        device = {"fs_0": ahead(pos), "fs_1": cc}
        return (
            remote(gate_ref.at[e, g_rows], gate_v.at[me, g_rows], gu_s.at[0], gu_r.at[pos, c, 0], device),
            remote(up_ref.at[e, g_rows], up_v.at[me, g_rows], gu_s.at[0], gu_r.at[pos, c, 1], device),
        )

    def down_copies(pos, c):
        cc = lax.rem(core + c, 2)
        e = ahead(pos) * 2 + cc
        device = {"fs_0": ahead(pos), "fs_1": cc}
        return (remote(down_ref.at[e, d_rows], down_v.at[me, d_rows], dn_s.at[0], dn_r.at[pos, c], device),)

    def send_weights(copies_of):
        for pos in range(1, n_z - 1):
            for c in range(2):
                for copy in copies_of(pos, c):
                    copy.start()

        @pl.when(jnp.logical_not(relays))
        def _():
            for c in range(2):
                for copy in copies_of(opposite, c):
                    copy.start()

    def send_gate_up():
        @pl.when(relays)
        def _():
            for c in range(2):
                e = ahead(opposite) * 2 + c
                first_leg(1 + 2 * c, gate_ref.at[e, g_rows], stage_gu.at[c, 0])
                first_leg(2 + 2 * c, up_ref.at[e, g_rows], stage_gu.at[c, 1])

        send_weights(gate_up_copies)

    def relay_gate_up():
        @pl.when(relays)
        def _():
            for c in range(2):
                n = 1 - c
                second_leg(
                    1 + 2 * c, stage_gu.at[c, 0], gate_v.at[origin, g_rows], gu_r.at[opposite, n, 0], leg_dest(c)
                )
                second_leg(2 + 2 * c, stage_gu.at[c, 1], up_v.at[origin, g_rows], gu_r.at[opposite, n, 1], leg_dest(c))

    def send_down():
        @pl.when(relays)
        def _():
            for c in range(2):
                first_leg(5 + c, down_ref.at[ahead(opposite) * 2 + c, d_rows], stage_dn.at[c])

        send_weights(down_copies)

    def relay_down():
        @pl.when(relays)
        def _():
            for c in range(2):
                second_leg(5 + c, stage_dn.at[c], down_v.at[origin, d_rows], dn_r.at[opposite, 1 - c], leg_dest(c))

    def relay_back():
        @pl.when(relays)
        def _():
            second_leg(7, stage_x.at[1], ret_ref.at[0, opposite], ret_r.at[opposite], leg)

    def wait_tokens(k):
        for pos in range(k * per, (k + 1) * per):
            if pos:
                got(x_buf.at[0, pos], tok_r.at[pos])

    def hop(buf, k, h, s_sems, r_sems):
        whole = pl.ds(k * per, per)
        first_half, second_half = pl.ds(k * per, per // 2), pl.ds(k * per + per // 2, per // 2)
        last = n_x // 2
        if h > 1:
            arrived(buf, k, h - 1, r_sems)
        rows = first_half if h == last else whole
        send(buf.at[h - 1, rows], buf.at[h, rows], s_sems.at[0], r_sems.at[k, h - 1, 0], right)
        rows = second_half if h == last else whole
        send(buf.at[(n_x - h + 1) % n_x, rows], buf.at[n_x - h, rows], s_sems.at[0], r_sems.at[k, h - 1, 1], left)

    def arrived(buf, k, h, r_sems):
        last = n_x // 2
        whole = pl.ds(k * per, per)
        first_half, second_half = pl.ds(k * per, per // 2), pl.ds(k * per + per // 2, per // 2)
        got(buf.at[h, first_half if h == last else whole], r_sems.at[k, h - 1, 0])
        got(buf.at[n_x - h, second_half if h == last else whole], r_sems.at[k, h - 1, 1])

    def forward_gu(k):
        for pos in range(max(1, k * per), (k + 1) * per):
            for c in range(2):
                cc = lax.rem(core + c, 2)
                s = behind(pos) * 2 + cc
                got(gate_v.at[s, g_rows], gu_r.at[pos, c, 0])
                got(up_v.at[s, g_rows], gu_r.at[pos, c, 1])
            pair = pl.ds(behind(pos) * 2, 2)
            send(gate_v.at[pair, g_rows], gate_v.at[pair, g_rows], ygu_s.at[0], ygu_r.at[pos, 0], y_peer)
            send(up_v.at[pair, g_rows], up_v.at[pair, g_rows], ygu_s.at[0], ygu_r.at[pos, 1], y_peer)

    def forward_dn(k):
        for pos in range(max(1, k * per), (k + 1) * per):
            for c in range(2):
                cc = lax.rem(core + c, 2)
                got(down_v.at[behind(pos) * 2 + cc, d_rows], dn_r.at[pos, c])
            pair = pl.ds(behind(pos) * 2, 2)
            send(down_v.at[pair, d_rows], down_v.at[pair, d_rows], ydn_s.at[0], ydn_r.at[pos], y_peer)

    def build_picks():
        chosen = []
        for k in range(2):
            e = route_ref[k : k + 1, :]
            far = lax.rem(e // 2 - z + n_z, n_z)
            pos = jnp.where(far == 0, 0, jnp.where(far <= n_z // 2, 2 * far - 1, 2 * (n_z - far)))
            crossed = jnp.where(lax.rem(e, 2) == core, 0, 1)
            inside = jnp.sum(names[k] * place, axis=0, keepdims=True)
            chosen.append((crossed * (n_z * slot + CAP) + pos * slot).astype(f32) + inside)
        chosen += [mix_ref[0:1, :], mix_ref[1:2, :]]
        table = jnp.concatenate(chosen + [jnp.zeros((128 - len(chosen), n_tok), f32)], axis=0).T
        step = per * slot
        for c in range(2 * CHUNKS):
            ids = (lax.broadcasted_iota(jnp.int32, (n_tok, step), 1) + c * step).astype(f32)
            w = jnp.where(ids == table[:, 0:1], table[:, 2:3], 0.0) + jnp.where(ids == table[:, 1:2], table[:, 3:4], 0.0)
            hi = w.astype(bf16)
            pick_hi[c] = hi
            pick_lo[c] = (w - hi.astype(f32)).astype(bf16)

    def hop_x(k, h):
        if h == 1:
            wait_tokens(k)
        hop(x_buf, k, h, xs, xr)

    top = n_x // 2
    begins = (0, 0, 1, 2, 2, 3, 4, 5)
    gate_up_rounds = {6: (0, 1, 2), 7: (3, 4, 5, 6), 8: (7,)}
    for r in range(begins[-1] + top):
        for k in range(CHUNKS):
            if 0 <= r - begins[k] < top:
                hop_x(k, r - begins[k] + 1)
        if r == 1:
            relay_tokens()
            send_gate_up()
        if r == 2:
            build_picks()
        if r == 5:
            relay_gate_up()
            send_down()
        for k in gate_up_rounds.get(r, ()):
            forward_gu(k)

    relay_down()

    o_g_rows = pl.ds(pl.multiple_of((1 - half) * g_half, g_half), g_half)
    o_d_rows = pl.ds(pl.multiple_of((1 - half) * d_half, d_half), d_half)
    got(gate_v.at[mate], gu_r.at[0, 0, 0])
    got(up_v.at[mate], gu_r.at[0, 0, 1])
    for pos in range(1, n_z):
        pair = pl.ds(behind(pos) * 2, 2)
        got(gate_v.at[pair, o_g_rows], ygu_r.at[pos, 0])
        got(up_v.at[pair, o_g_rows], ygu_r.at[pos, 1])
    outs = [
        pltpu.make_async_copy(gate_v, gate_out, out_sem.at[0]),
        pltpu.make_async_copy(up_v, up_out, out_sem.at[1]),
        pltpu.make_async_copy(down_v, down_out, out_sem.at[2]),
    ]
    outs[0].start()
    outs[1].start()

    def wait_down():
        got(down_v.at[mate], dn_r.at[0, 0])
        for pos in range(1, n_z):
            got(down_v.at[pl.ds(behind(pos) * 2, 2), o_d_rows], ydn_r.at[pos])
        outs[2].start()

    f_src = 2 * n_z // n_x
    rows = per * slot

    def expert_hidden(k):
        arrived(x_buf, k, n_x // 2, xr)
        total = jnp.zeros((rows, 2 * gate_v.shape[2]), jnp.float32)
        square = jnp.zeros((rows, width), jnp.float32)
        for s in range(n_x):
            t = lax.rem(x + n_x - s, n_x)
            block = x_buf[s, k * per : (k + 1) * per].reshape(rows, width)
            src = pl.ds(t * f_src, f_src)
            w = jnp.concatenate(
                [gate_v[src].reshape(width, gate_v.shape[2]), up_v[src].reshape(width, up_v.shape[2])], axis=1
            )
            total = total + jnp.dot(block, w, preferred_element_type=jnp.float32)
            wide = block.astype(jnp.float32)
            square = square + wide * wide
        scale = lax.rsqrt(jnp.sum(square, axis=1, keepdims=True) * (1.0 / (n_x * width)) + EPSILON)
        n_h = gate_v.shape[2]
        g = total[:, :n_h] * scale
        u = total[:, n_h:] * scale
        hidden = (g / (1.0 + jnp.exp(-g))) * u
        h_buf[0, k * per : (k + 1) * per] = hidden.astype(jnp.bfloat16).reshape(per, slot, n_h)

    def hop_h(k, h):
        hop(h_buf, k, h, hs, hr)

    def expert_out(k):
        arrived(h_buf, k, n_x // 2, hr)
        n_h = h_buf.shape[3]
        total = jnp.zeros((rows, width), jnp.float32)
        for s in range(n_x):
            t = lax.rem(x + n_x - s, n_x)
            w = down_v[pl.ds(t * f_src, f_src)].reshape(n_h, width)
            block = h_buf[s, k * per : (k + 1) * per].reshape(rows, n_h)
            total = total + jnp.dot(block, w, preferred_element_type=jnp.float32)
        o_buf[k * per : (k + 1) * per] = total.astype(jnp.bfloat16).reshape(per, slot, width)

    def send_out(k):
        for pos in reversed(range(k * per, (k + 1) * per)):
            if pos:
                copy = remote(o_buf.at[pos], ret_ref.at[0, pos], ret_s.at[0], ret_r.at[pos], {"fs_0": behind(pos)})
                if pos < opposite:
                    copy.start()
                    continue

                @pl.when(relays)
                def _():
                    first_leg(7, o_buf.at[pos], stage_x.at[1])

                @pl.when(jnp.logical_not(relays))
                def _():
                    copy.start()
            else:
                ret_ref[0, 0] = o_buf[0]

    near, far = tuple(range(CHUNKS // 2 - 1, -1, -1)), tuple(range(CHUNKS - 1, CHUNKS // 2 - 1, -1))

    def hops(chunks, h):
        for k in chunks:
            if h == 1:
                expert_hidden(k)
            hop_h(k, h)

    def finish(chunks):
        for k in chunks:
            expert_out(k)
            send_out(k)

    hops(far, 1)
    for k in range(0, 5):
        forward_dn(k)
    hops(far, 2)
    forward_dn(5)
    hops(near, 1)
    hops(far, 3)
    forward_dn(6)
    forward_dn(7)
    hops(far, 4)
    hops(near, 2)
    wait_down()
    finish(far[:2])
    hops(near, 3)
    finish(far[2:])
    relay_back()
    hops(near, 4)
    finish(near)
    first.wait_send()
    serving = n_z * 2
    got(x_buf.at[pl.ds(0, n_x - 1)], xs.at[0])
    got(h_buf.at[pl.ds(0, n_x - 1)], hs.at[0])
    got(gate_v.at[pl.ds(0, serving - 2)], ygu_s.at[0])
    got(down_v.at[pl.ds(0, n_z - 1)], ydn_s.at[0])

    @pl.when(relays)
    def _():
        got(comb.at[pl.ds(0, n_z - 2)], tok_s.at[0])
        got(gate_v.at[pl.ds(0, serving - 2)], gu_s.at[0])
        got(down_v.at[pl.ds(0, n_z - 1)], dn_s.at[0])

    @pl.when(jnp.logical_not(relays))
    def _():
        got(comb.at[pl.ds(0, n_z - 1)], tok_s.at[0])
        got(gate_v, gu_s.at[0])
        got(down_v.at[pl.ds(0, n_z)], dn_s.at[0])

    outs[0].wait()
    outs[1].wait()
    outs[2].wait()

    def mixed(c, k):
        data = ret_ref[c, k * per : (k + 1) * per].reshape(rows, width)
        part = jnp.dot(pick_hi[c * CHUNKS + k], data, preferred_element_type=f32)
        return part + jnp.dot(pick_lo[c * CHUNKS + k], data, preferred_element_type=f32)

    total = jnp.zeros((n_tok, width), f32)
    backs = tuple(reversed(range(CHUNKS)))
    for n, k in enumerate(backs):
        for pos in range(k * per, (k + 1) * per):
            if pos:
                got(ret_ref.at[0, pos], ret_r.at[pos])
        part = pl.ds(k * per, per)
        copy = remote(ret_ref.at[0, part], ret_ref.at[1, part], fin_s.at[0], fin_r.at[k], other_core)
        copy.start()
        total = total + mixed(0, k)
        if n:
            got(ret_ref.at[1, pl.ds(backs[n - 1] * per, per)], fin_r.at[backs[n - 1]])
            total = total + mixed(1, backs[n - 1])
    got(ret_ref.at[1, pl.ds(backs[-1] * per, per)], fin_r.at[backs[-1]])
    total = total + mixed(1, backs[-1])
    mixture_ref[...] = total.astype(bf16)
    got(ret_ref.at[0], fin_s.at[0])

    @pl.when(relays)
    def _():
        got(o_buf.at[pl.ds(0, n_z - 2)], ret_s.at[0])
        for n in range(2):
            got(stage_x.at[0], stage_s.at[0, n])
            got(stage_x.at[1], stage_s.at[7, n])
            for c in range(2):
                got(stage_gu.at[c, 0], stage_s.at[1 + 2 * c, n])
                got(stage_gu.at[c, 1], stage_s.at[2 + 2 * c, n])
                got(stage_dn.at[c], stage_s.at[5 + c, n])

    @pl.when(jnp.logical_not(relays))
    def _():
        got(o_buf.at[pl.ds(0, n_z - 1)], ret_s.at[0])


def exchange_and_apply(tokens, routes, mix, gain, gate, up, down, sizes):
    n_z, n_x, n_grp = sizes
    f32, bf16 = jnp.float32, jnp.bfloat16
    n_tok, width = tokens.shape
    slot = 2 * CAP
    n_h = gate.shape[2]
    experts = gate.shape[0]
    dma = pltpu.SemaphoreType.DMA
    hops = n_x // 2
    vmem = pl.BlockSpec(memory_space=pltpu.VMEM)
    hbm = pl.BlockSpec(memory_space=pl.ANY)
    picks = (2 * CHUNKS, n_tok, n_z // CHUNKS * slot)
    return pl.pallas_call(
        functools.partial(kernel, sizes),
        out_shape=(
            jax.ShapeDtypeStruct(gate.shape, bf16),
            jax.ShapeDtypeStruct(up.shape, bf16),
            jax.ShapeDtypeStruct(down.shape, bf16),
            jax.ShapeDtypeStruct(tokens.shape, bf16),
        ),
        in_specs=[vmem] * 4 + [hbm] * 3,
        out_specs=(hbm, hbm, hbm, vmem),
        scratch_shapes=[
            pltpu.VMEM((2,) + gate.shape, f32),
            pltpu.VMEM(down.shape, f32),
            pltpu.VMEM(gate.shape, bf16),
            pltpu.VMEM(up.shape, bf16),
            pltpu.VMEM(down.shape, bf16),
            pltpu.VMEM((experts, n_tok), f32),
            pltpu.VMEM(picks, bf16),
            pltpu.VMEM(picks, bf16),
            pltpu.VMEM((2, n_z, slot, width), bf16),
            pltpu.VMEM((2, n_z, slot, width), bf16),
            pltpu.VMEM((n_z, slot, width), bf16),
            pltpu.VMEM((n_z, slot, width), bf16),
            pltpu.VMEM((n_x, n_z, slot, width), bf16),
            pltpu.VMEM((n_x, n_z, slot, n_h), bf16),
            pltpu.VMEM((n_z, slot, width), bf16),
            pltpu.VMEM(gate.shape, bf16),
            pltpu.VMEM(up.shape, bf16),
            pltpu.VMEM(down.shape, bf16),
            dma((2,)),
            dma((1,)),
            dma((n_z,)),
            dma((1,)),
            dma((n_z, 2, 2)),
            dma((1,)),
            dma((n_z, 2)),
            dma((1,)),
            dma((n_z, 2)),
            dma((1,)),
            dma((n_z,)),
            dma((1,)),
            dma((CHUNKS, hops, 2)),
            dma((1,)),
            dma((CHUNKS, hops, 2)),
            dma((1,)),
            dma((n_z,)),
            dma((1,)),
            dma((CHUNKS,)),
            dma((3,)),
            dma((3,)),
            pltpu.VMEM((2, slot, width), bf16),
            pltpu.VMEM((2, 2, gate.shape[1] // 2, n_h), bf16),
            pltpu.VMEM((2, down.shape[1] // 2, width), bf16),
            dma((8, 2)),
            dma((8,)),
        ],
        compiler_params=pltpu.CompilerParams(
            collective_id=0, has_side_effects=True, vmem_limit_bytes=67043328
        ),
        name="exchange_and_apply",
    )(tokens, routes, mix, gain, gate, up, down)


def put_out(*refs):
    n = (len(refs) - 1) // 3
    ins, outs, held, sems = refs[:n], refs[n : 2 * n], refs[2 * n : 3 * n], refs[3 * n]
    reads = [pltpu.make_async_copy(ins[i], held[i], sems.at[0, i]) for i in range(n)]
    writes = [pltpu.make_async_copy(held[i], outs[i], sems.at[1, i]) for i in range(n)]
    for copy in reads:
        copy.start()
    for read, write in zip(reads, writes):
        read.wait()
        write.start()
    for copy in writes:
        copy.wait()


def outputs(arrays):
    hbm = pl.BlockSpec(memory_space=pl.ANY)
    return pl.pallas_call(
        put_out,
        out_shape=tuple(jax.ShapeDtypeStruct(a.shape, a.dtype) for a in arrays),
        in_specs=[hbm] * len(arrays),
        out_specs=tuple([hbm] * len(arrays)),
        scratch_shapes=[pltpu.VMEM(a.shape, a.dtype) for a in arrays]
        + [pltpu.SemaphoreType.DMA((2, len(arrays)))],
        compiler_params=pltpu.CompilerParams(vmem_limit_bytes=67043328),
        name="outputs",
    )(*arrays)


def shards(tokens, norm_gain, gate_weight, up_weight, down_weight, routes, route_weights):
    sizes = (lax.axis_size("fs_0"), lax.axis_size("tp"), lax.axis_size("grp"))
    gate_serve, up_serve, down_serve, mixture = outputs(
        exchange_and_apply(
            tokens, routes.T, route_weights.T, norm_gain[None, :], gate_weight, up_weight, down_weight, sizes
        )
    )
    return (
        gate_serve.reshape(1, -1, gate_serve.shape[2]),
        up_serve.reshape(1, -1, up_serve.shape[2]),
        down_serve.reshape(1, -1, down_serve.shape[2]),
        mixture,
    )


def solution(mesh):
    split = Mesh(
        mesh.devices.reshape(mesh.shape["grp"], mesh.shape["fs"] // 2, 2, mesh.shape["tp"]),
        ("grp", "fs_0", "fs_1", "tp"),
    )
    placed = (
        P(GRP_FS, "tp"),
        P(FS),
        P(None, FS, "tp"),
        P(None, FS, "tp"),
        P(None, FS, "tp"),
        P(GRP_FS, None),
        P(GRP_FS, None),
    )
    return jax.shard_map(
        shards,
        mesh=split,
        in_specs=placed,
        out_specs=(
            P(GRP_FS, None, "tp"),
            P(GRP_FS, None, "tp"),
            P(GRP_FS, None, "tp"),
            P(GRP_FS, "tp"),
        ),
        check_vma=False,
    )
```

```python
import functools

import jax
import jax.numpy as jnp
from jax import lax
from jax.experimental import pallas as pl
from jax.experimental.pallas import tpu as pltpu
from jax.sharding import Mesh
from jax.sharding import PartitionSpec as P

CAP = 36
FS = ("fs_0", "fs_1")
GRP_FS = ("grp", "fs_0", "fs_1")
MESH = pl.DeviceIdType.MESH
EPSILON = 1e-06
CHUNKS = 8


def ring_order(n):
    order = [0]
    for d in range(1, n // 2 + 1):
        order.append(d)
        if len(order) < n:
            order.append(n - d)
    return order


def kernel(
    sizes,
    tok_ref,
    route_ref,
    mix_ref,
    gain_ref,
    gate_in,
    up_in,
    down_in,
    gate_out,
    up_out,
    down_out,
    mixture_ref,
    wide_v,
    wide_d,
    gate_ref,
    up_ref,
    down_ref,
    place_v,
    pick_hi,
    pick_lo,
    outb_ref,
    ret_ref,
    swap,
    comb,
    x_buf,
    h_buf,
    o_buf,
    gate_v,
    up_v,
    down_v,
    swap_sems,
    tok_s,
    tok_r,
    gu_s,
    gu_r,
    dn_s,
    dn_r,
    ygu_s,
    ygu_r,
    ydn_s,
    ydn_r,
    xs,
    xr,
    hs,
    hr,
    ret_s,
    ret_r,
    fin_s,
    fin_r,
    out_sem,
    in_sem,
    stage_x,
    stage_gu,
    stage_dn,
    stage_s,
    stage_r,
):
    n_z, n_x, n_grp = sizes
    order = ring_order(n_z)
    per = n_z // CHUNKS
    slot, width = x_buf.shape[2], x_buf.shape[3]
    g_half = gate_v.shape[1] // 2
    d_half = down_v.shape[1] // 2
    grp = lax.axis_index("grp")
    z = lax.axis_index("fs_0")
    core = lax.axis_index("fs_1")
    x = lax.axis_index("tp")
    me = z * 2 + core
    half = lax.rem(grp, 2)
    y_peer = {"grp": grp + 1 - 2 * half}
    other_core = {"fs_1": 1 - core}
    right = {"tp": lax.rem(x + 1, n_x)}
    left = {"tp": lax.rem(x + n_x - 1, n_x)}

    def ahead(pos):
        return lax.rem(z + order[pos], n_z)

    def behind(pos):
        return lax.rem(z + n_z - order[pos], n_z)

    def remote(src, dst, send_sem, recv_sem, device):
        return pltpu.make_async_remote_copy(
            src_ref=src, dst_ref=dst, send_sem=send_sem, recv_sem=recv_sem, device_id=device, device_id_type=MESH
        )

    def send(*args):
        copy = remote(*args)
        copy.start()
        return copy

    barrier = pltpu.get_barrier_semaphore()
    peers = [y_peer, other_core, right, left]
    for pos in range(1, n_z):
        for c in range(2):
            peers.append({"fs_0": ahead(pos), "fs_1": c})
    for device in peers:
        pl.semaphore_signal(barrier, inc=1, device_id=device, device_id_type=MESH)

    loads = [
        pltpu.make_async_copy(gate_in, wide_v.at[0], in_sem.at[0]),
        pltpu.make_async_copy(up_in, wide_v.at[1], in_sem.at[1]),
        pltpu.make_async_copy(down_in, wide_d, in_sem.at[2]),
    ]
    for copy in loads:
        copy.start()

    f32, bf16 = jnp.float32, jnp.bfloat16
    n_tok = tok_ref.shape[0]
    experts = 2 * n_z
    expert_ids = lax.broadcasted_iota(jnp.int32, (experts, n_tok), 0)
    names = [jnp.where(expert_ids == route_ref[k : k + 1, :], 1.0, 0.0) for k in range(2)]
    named = names[0] + names[1]
    before = lax.broadcasted_iota(jnp.int32, (n_tok, n_tok), 0) < lax.broadcasted_iota(jnp.int32, (n_tok, n_tok), 1)
    before = jnp.where(before, 1.0, 0.0).astype(bf16)
    place = jnp.dot(named.astype(bf16), before, preferred_element_type=f32)
    place_v[...] = jnp.where(named > 0.5, place, -1.0 - slot)

    def dispatch(j, crossed):
        distance = jnp.where(lax.rem(j, 2) == 1, (j + 1) // 2, n_z - j // 2)
        e = lax.rem(z + distance, n_z) * 2 + jnp.where(crossed == 1, 1 - core, core)
        slot_ids = lax.broadcasted_iota(jnp.int32, (slot, n_tok), 0).astype(f32) - CAP * crossed
        pick = jnp.where(slot_ids == place_v[pl.ds(e, 1), :], 1.0, 0.0).astype(bf16)
        outb_ref[crossed, j] = jnp.dot(pick, tok_ref[...], preferred_element_type=f32).astype(bf16)

    def dispatch_both(j, carry):
        dispatch(j, 1)
        dispatch(j, 0)
        return carry

    lax.fori_loop(0, n_z, dispatch_both, 0)
    pl.semaphore_wait(barrier, len(peers))

    first = send(outb_ref.at[1], swap, swap_sems.at[0], swap_sems.at[1], other_core)

    n_gain = gain_ref.shape[1]
    eye = lax.broadcasted_iota(jnp.int32, (n_gain, n_gain), 0) == lax.broadcasted_iota(jnp.int32, (n_gain, n_gain), 1)
    gain = jnp.sum(jnp.where(eye, gain_ref[...], 0.0), axis=1, keepdims=True)
    for copy in loads:
        copy.wait()

    def cast(e, carry):
        gate_ref[e] = (gain * wide_v[0, e]).astype(bf16)
        up_ref[e] = (gain * wide_v[1, e]).astype(bf16)
        down_ref[e] = wide_d[e].astype(bf16)
        return carry

    lax.fori_loop(0, experts, cast, 0)

    first.wait_recv()
    comb[...] = outb_ref[0] + swap[...]
    x_buf[0, 0] = outb_ref[0, 0] + swap[0]
    gate_v[me] = gate_ref[me]
    up_v[me] = up_ref[me]
    down_v[me] = down_ref[me]

    opposite = n_z - 1
    leg = {"fs_0": lax.rem(z + n_z - n_z // 4, n_z)}
    origin = lax.rem(z + n_z // 4, n_z) * 2 + 1
    relays = core == 1

    def leg_dest(c):
        return {"fs_0": lax.rem(z + n_z - n_z // 4, n_z), "fs_1": c}

    def first_leg(n, src, stage):
        remote(src, stage, stage_s.at[n, 0], stage_r.at[n], leg).start()

    def second_leg(n, stage, dst, recv_sem, device):
        got(stage, stage_r.at[n])
        remote(stage, dst, stage_s.at[n, 1], recv_sem, device).start()

    def got(ref, sem):
        pltpu.make_async_copy(ref, ref, sem).wait()

    @pl.when(relays)
    def _():
        first_leg(0, comb.at[opposite], stage_x.at[0])

    for pos in range(1, n_z - 1):
        send(comb.at[pos], x_buf.at[0, pos], tok_s.at[0], tok_r.at[pos], {"fs_0": ahead(pos)})

    @pl.when(jnp.logical_not(relays))
    def _():
        remote(
            comb.at[opposite], x_buf.at[0, opposite], tok_s.at[0], tok_r.at[opposite], {"fs_0": ahead(opposite)}
        ).start()

    def relay_tokens():
        @pl.when(relays)
        def _():
            second_leg(0, stage_x.at[0], x_buf.at[0, opposite], tok_r.at[opposite], leg)

    g_rows = pl.ds(pl.multiple_of(half * g_half, g_half), g_half)
    d_rows = pl.ds(pl.multiple_of(half * d_half, d_half), d_half)
    mate = z * 2 + 1 - core
    send(gate_ref.at[mate], gate_v.at[me], gu_s.at[0], gu_r.at[0], other_core)
    send(up_ref.at[mate], up_v.at[me], gu_s.at[0], gu_r.at[0], other_core)
    send(down_ref.at[mate], down_v.at[me], dn_s.at[0], dn_r.at[0], other_core)
    def gate_up_copies(pos, c):
        cc = lax.rem(core + c, 2)
        e = ahead(pos) * 2 + cc
        device = {"fs_0": ahead(pos), "fs_1": cc}
        return (
            remote(gate_ref.at[e, g_rows], gate_v.at[me, g_rows], gu_s.at[0], gu_r.at[pos], device),
            remote(up_ref.at[e, g_rows], up_v.at[me, g_rows], gu_s.at[0], gu_r.at[pos], device),
        )

    def down_copies(pos, c):
        cc = lax.rem(core + c, 2)
        e = ahead(pos) * 2 + cc
        device = {"fs_0": ahead(pos), "fs_1": cc}
        return (remote(down_ref.at[e, d_rows], down_v.at[me, d_rows], dn_s.at[0], dn_r.at[pos], device),)

    def send_weights(copies_of):
        for pos in range(1, n_z - 1):
            for c in range(2):
                for copy in copies_of(pos, c):
                    copy.start()

        @pl.when(jnp.logical_not(relays))
        def _():
            for c in range(2):
                for copy in copies_of(opposite, c):
                    copy.start()

    def send_gate_up():
        @pl.when(relays)
        def _():
            for c in range(2):
                e = ahead(opposite) * 2 + c
                first_leg(1 + 2 * c, gate_ref.at[e, g_rows], stage_gu.at[c, 0])
                first_leg(2 + 2 * c, up_ref.at[e, g_rows], stage_gu.at[c, 1])

        send_weights(gate_up_copies)

    def relay_gate_up():
        @pl.when(relays)
        def _():
            for c in range(2):
                second_leg(
                    1 + 2 * c, stage_gu.at[c, 0], gate_v.at[origin, g_rows], gu_r.at[opposite], leg_dest(c)
                )
                second_leg(2 + 2 * c, stage_gu.at[c, 1], up_v.at[origin, g_rows], gu_r.at[opposite], leg_dest(c))

    def send_down():
        @pl.when(relays)
        def _():
            for c in range(2):
                first_leg(5 + c, down_ref.at[ahead(opposite) * 2 + c, d_rows], stage_dn.at[c])

        send_weights(down_copies)

    def relay_down():
        @pl.when(relays)
        def _():
            for c in range(2):
                second_leg(5 + c, stage_dn.at[c], down_v.at[origin, d_rows], dn_r.at[opposite], leg_dest(c))

    def relay_back():
        @pl.when(relays)
        def _():
            second_leg(7, stage_x.at[1], ret_ref.at[0, opposite], ret_r.at[opposite], leg)

    def wait_tokens(k):
        for pos in range(k * per, (k + 1) * per):
            if pos:
                got(x_buf.at[0, pos], tok_r.at[pos])

    def hop(buf, k, h, s_sems, r_sems):
        whole = pl.ds(k * per, per)
        first_half, second_half = pl.ds(k * per, per // 2), pl.ds(k * per + per // 2, per // 2)
        last = n_x // 2
        if h > 1:
            arrived(buf, k, h - 1, r_sems)
        rows = first_half if h == last else whole
        send(buf.at[h - 1, rows], buf.at[h, rows], s_sems.at[0], r_sems.at[k, h - 1], right)
        rows = second_half if h == last else whole
        send(buf.at[(n_x - h + 1) % n_x, rows], buf.at[n_x - h, rows], s_sems.at[0], r_sems.at[k, h - 1], left)

    def arrived(buf, k, h, r_sems):
        got(buf.at[0, pl.ds(0, per if h == n_x // 2 else 2 * per)], r_sems.at[k, h - 1])

    def forward_gu(k):
        for pos in range(max(1, k * per), (k + 1) * per):
            pair = pl.ds(behind(pos) * 2, 2)
            got(gate_v.at[pair], gu_r.at[pos])
            send(gate_v.at[pair, g_rows], gate_v.at[pair, g_rows], ygu_s.at[0], ygu_r.at[pos], y_peer)
            send(up_v.at[pair, g_rows], up_v.at[pair, g_rows], ygu_s.at[0], ygu_r.at[pos], y_peer)

    def forward_dn(k):
        for pos in range(max(1, k * per), (k + 1) * per):
            pair = pl.ds(behind(pos) * 2, 2)
            got(down_v.at[pair, d_rows], dn_r.at[pos])
            send(down_v.at[pair, d_rows], down_v.at[pair, d_rows], ydn_s.at[0], ydn_r.at[pos], y_peer)

    def build_picks():
        chosen = []
        for k in range(2):
            e = route_ref[k : k + 1, :]
            far = lax.rem(e // 2 - z + n_z, n_z)
            pos = jnp.where(far == 0, 0, jnp.where(far <= n_z // 2, 2 * far - 1, 2 * (n_z - far)))
            crossed = jnp.where(lax.rem(e, 2) == core, 0, 1)
            inside = jnp.sum(names[k] * place, axis=0, keepdims=True)
            chosen.append((crossed * (n_z * slot + CAP) + pos * slot).astype(f32) + inside)
        chosen += [mix_ref[0:1, :], mix_ref[1:2, :]]
        table = jnp.concatenate(chosen + [jnp.zeros((128 - len(chosen), n_tok), f32)], axis=0).T
        step = per * slot
        for c in range(2 * CHUNKS):
            ids = (lax.broadcasted_iota(jnp.int32, (n_tok, step), 1) + c * step).astype(f32)
            w = jnp.where(ids == table[:, 0:1], table[:, 2:3], 0.0) + jnp.where(ids == table[:, 1:2], table[:, 3:4], 0.0)
            hi = w.astype(bf16)
            pick_hi[c] = hi
            pick_lo[c] = (w - hi.astype(f32)).astype(bf16)

    def hop_x(k, h):
        if h == 1:
            wait_tokens(k)
        hop(x_buf, k, h, xs, xr)

    top = n_x // 2
    begins = (0, 0, 1, 2, 2, 3, 4, 5)
    gate_up_rounds = {6: (0, 1, 2), 7: (3, 4, 5, 6), 8: (7,)}
    for r in range(begins[-1] + top):
        for k in range(CHUNKS):
            if 0 <= r - begins[k] < top:
                hop_x(k, r - begins[k] + 1)
        if r == 1:
            relay_tokens()
            send_gate_up()
        if r == 2:
            build_picks()
        if r == 5:
            relay_gate_up()
            send_down()
        for k in gate_up_rounds.get(r, ()):
            forward_gu(k)

    relay_down()

    o_d_rows = pl.ds(pl.multiple_of((1 - half) * d_half, d_half), d_half)
    got(gate_v.at[pl.ds(z * 2, 2)], gu_r.at[0])
    for pos in range(1, n_z):
        pair = pl.ds(behind(pos) * 2, 2)
        got(gate_v.at[pair], ygu_r.at[pos])
    outs = [
        pltpu.make_async_copy(gate_v, gate_out, out_sem.at[0]),
        pltpu.make_async_copy(up_v, up_out, out_sem.at[1]),
        pltpu.make_async_copy(down_v, down_out, out_sem.at[2]),
    ]
    outs[0].start()
    outs[1].start()

    def wait_down():
        got(down_v.at[mate], dn_r.at[0])
        for pos in range(1, n_z):
            got(down_v.at[pl.ds(behind(pos) * 2, 2), o_d_rows], ydn_r.at[pos])
        outs[2].start()

    f_src = 2 * n_z // n_x
    rows = per * slot

    def expert_hidden(k):
        arrived(x_buf, k, n_x // 2, xr)
        total = jnp.zeros((rows, 2 * gate_v.shape[2]), jnp.float32)
        square = jnp.zeros((rows, width), jnp.float32)
        for s in range(n_x):
            t = lax.rem(x + n_x - s, n_x)
            block = x_buf[s, k * per : (k + 1) * per].reshape(rows, width)
            src = pl.ds(t * f_src, f_src)
            w = jnp.concatenate(
                [gate_v[src].reshape(width, gate_v.shape[2]), up_v[src].reshape(width, up_v.shape[2])], axis=1
            )
            total = total + jnp.dot(block, w, preferred_element_type=jnp.float32)
            wide = block.astype(jnp.float32)
            square = square + wide * wide
        scale = lax.rsqrt(jnp.sum(square, axis=1, keepdims=True) * (1.0 / (n_x * width)) + EPSILON)
        n_h = gate_v.shape[2]
        g = total[:, :n_h] * scale
        u = total[:, n_h:] * scale
        hidden = (g / (1.0 + jnp.exp(-g))) * u
        h_buf[0, k * per : (k + 1) * per] = hidden.astype(jnp.bfloat16).reshape(per, slot, n_h)

    def hop_h(k, h):
        hop(h_buf, k, h, hs, hr)

    def expert_out(k):
        arrived(h_buf, k, n_x // 2, hr)
        n_h = h_buf.shape[3]
        total = jnp.zeros((rows, width), jnp.float32)
        for s in range(n_x):
            t = lax.rem(x + n_x - s, n_x)
            w = down_v[pl.ds(t * f_src, f_src)].reshape(n_h, width)
            block = h_buf[s, k * per : (k + 1) * per].reshape(rows, n_h)
            total = total + jnp.dot(block, w, preferred_element_type=jnp.float32)
        o_buf[k * per : (k + 1) * per] = total.astype(jnp.bfloat16).reshape(per, slot, width)

    def send_out(k):
        for pos in reversed(range(k * per, (k + 1) * per)):
            if pos:
                copy = remote(o_buf.at[pos], ret_ref.at[0, pos], ret_s.at[0], ret_r.at[pos], {"fs_0": behind(pos)})
                if pos < opposite:
                    copy.start()
                    continue

                @pl.when(relays)
                def _():
                    first_leg(7, o_buf.at[pos], stage_x.at[1])

                @pl.when(jnp.logical_not(relays))
                def _():
                    copy.start()
            else:
                ret_ref[0, 0] = o_buf[0]

    near, far = tuple(range(CHUNKS // 2 - 1, -1, -1)), tuple(range(CHUNKS - 1, CHUNKS // 2 - 1, -1))

    def hops(chunks, h):
        for k in chunks:
            if h == 1:
                expert_hidden(k)
            hop_h(k, h)

    def finish(chunks):
        for k in chunks:
            expert_out(k)
            send_out(k)

    hops(far, 1)
    for k in range(0, 5):
        forward_dn(k)
    hops(far, 2)
    forward_dn(5)
    hops(near, 1)
    hops(far, 3)
    forward_dn(6)
    forward_dn(7)
    hops(far, 4)
    hops(near, 2)
    wait_down()
    finish(far[:2])
    hops(near, 3)
    finish(far[2:])
    relay_back()
    hops(near, 4)
    finish(near)
    first.wait_send()
    serving = n_z * 2
    got(x_buf.at[pl.ds(0, n_x - 1)], xs.at[0])
    got(h_buf.at[pl.ds(0, n_x - 1)], hs.at[0])
    got(gate_v.at[pl.ds(0, serving - 2)], ygu_s.at[0])
    got(down_v.at[pl.ds(0, n_z - 1)], ydn_s.at[0])

    @pl.when(relays)
    def _():
        got(comb.at[pl.ds(0, n_z - 2)], tok_s.at[0])
        got(gate_v.at[pl.ds(0, serving - 2)], gu_s.at[0])
        got(down_v.at[pl.ds(0, n_z - 1)], dn_s.at[0])

    @pl.when(jnp.logical_not(relays))
    def _():
        got(comb.at[pl.ds(0, n_z - 1)], tok_s.at[0])
        got(gate_v, gu_s.at[0])
        got(down_v.at[pl.ds(0, n_z)], dn_s.at[0])

    outs[0].wait()
    outs[1].wait()
    outs[2].wait()

    def mixed(c, k):
        data = ret_ref[c, k * per : (k + 1) * per].reshape(rows, width)
        part = jnp.dot(pick_hi[c * CHUNKS + k], data, preferred_element_type=f32)
        return part + jnp.dot(pick_lo[c * CHUNKS + k], data, preferred_element_type=f32)

    total = jnp.zeros((n_tok, width), f32)
    backs = tuple(reversed(range(CHUNKS)))
    for n, k in enumerate(backs):
        for pos in range(k * per, (k + 1) * per):
            if pos:
                got(ret_ref.at[0, pos], ret_r.at[pos])
        part = pl.ds(k * per, per)
        copy = remote(ret_ref.at[0, part], ret_ref.at[1, part], fin_s.at[0], fin_r.at[k], other_core)
        copy.start()
        total = total + mixed(0, k)
        if n:
            got(ret_ref.at[1, pl.ds(backs[n - 1] * per, per)], fin_r.at[backs[n - 1]])
            total = total + mixed(1, backs[n - 1])
    got(ret_ref.at[1, pl.ds(backs[-1] * per, per)], fin_r.at[backs[-1]])
    total = total + mixed(1, backs[-1])
    mixture_ref[...] = total.astype(bf16)
    got(ret_ref.at[0], fin_s.at[0])

    @pl.when(relays)
    def _():
        got(o_buf.at[pl.ds(0, n_z - 2)], ret_s.at[0])
        for n in range(2):
            got(stage_x.at[0], stage_s.at[0, n])
            got(stage_x.at[1], stage_s.at[7, n])
            for c in range(2):
                got(stage_gu.at[c, 0], stage_s.at[1 + 2 * c, n])
                got(stage_gu.at[c, 1], stage_s.at[2 + 2 * c, n])
                got(stage_dn.at[c], stage_s.at[5 + c, n])

    @pl.when(jnp.logical_not(relays))
    def _():
        got(o_buf.at[pl.ds(0, n_z - 1)], ret_s.at[0])


def exchange_and_apply(tokens, routes, mix, gain, gate, up, down, sizes):
    n_z, n_x, n_grp = sizes
    f32, bf16 = jnp.float32, jnp.bfloat16
    n_tok, width = tokens.shape
    slot = 2 * CAP
    n_h = gate.shape[2]
    experts = gate.shape[0]
    dma = pltpu.SemaphoreType.DMA
    hops = n_x // 2
    vmem = pl.BlockSpec(memory_space=pltpu.VMEM)
    hbm = pl.BlockSpec(memory_space=pl.ANY)
    picks = (2 * CHUNKS, n_tok, n_z // CHUNKS * slot)
    return pl.pallas_call(
        functools.partial(kernel, sizes),
        out_shape=(
            jax.ShapeDtypeStruct(gate.shape, bf16),
            jax.ShapeDtypeStruct(up.shape, bf16),
            jax.ShapeDtypeStruct(down.shape, bf16),
            jax.ShapeDtypeStruct(tokens.shape, bf16),
        ),
        in_specs=[vmem] * 4 + [hbm] * 3,
        out_specs=(hbm, hbm, hbm, vmem),
        scratch_shapes=[
            pltpu.VMEM((2,) + gate.shape, f32),
            pltpu.VMEM(down.shape, f32),
            pltpu.VMEM(gate.shape, bf16),
            pltpu.VMEM(up.shape, bf16),
            pltpu.VMEM(down.shape, bf16),
            pltpu.VMEM((experts, n_tok), f32),
            pltpu.VMEM(picks, bf16),
            pltpu.VMEM(picks, bf16),
            pltpu.VMEM((2, n_z, slot, width), bf16),
            pltpu.VMEM((2, n_z, slot, width), bf16),
            pltpu.VMEM((n_z, slot, width), bf16),
            pltpu.VMEM((n_z, slot, width), bf16),
            pltpu.VMEM((n_x, n_z, slot, width), bf16),
            pltpu.VMEM((n_x, n_z, slot, n_h), bf16),
            pltpu.VMEM((n_z, slot, width), bf16),
            pltpu.VMEM(gate.shape, bf16),
            pltpu.VMEM(up.shape, bf16),
            pltpu.VMEM(down.shape, bf16),
            dma((2,)),
            dma((1,)),
            dma((n_z,)),
            dma((1,)),
            dma((n_z,)),
            dma((1,)),
            dma((n_z,)),
            dma((1,)),
            dma((n_z,)),
            dma((1,)),
            dma((n_z,)),
            dma((1,)),
            dma((CHUNKS, hops)),
            dma((1,)),
            dma((CHUNKS, hops)),
            dma((1,)),
            dma((n_z,)),
            dma((1,)),
            dma((CHUNKS,)),
            dma((3,)),
            dma((3,)),
            pltpu.VMEM((2, slot, width), bf16),
            pltpu.VMEM((2, 2, gate.shape[1] // 2, n_h), bf16),
            pltpu.VMEM((2, down.shape[1] // 2, width), bf16),
            dma((8, 2)),
            dma((8,)),
        ],
        compiler_params=pltpu.CompilerParams(
            collective_id=0, has_side_effects=True, vmem_limit_bytes=67043328
        ),
        name="exchange_and_apply",
    )(tokens, routes, mix, gain, gate, up, down)


def put_out(*refs):
    n = (len(refs) - 1) // 3
    ins, outs, held, sems = refs[:n], refs[n : 2 * n], refs[2 * n : 3 * n], refs[3 * n]
    reads = [pltpu.make_async_copy(ins[i], held[i], sems.at[0, i]) for i in range(n)]
    writes = [pltpu.make_async_copy(held[i], outs[i], sems.at[1, i]) for i in range(n)]
    for copy in reads:
        copy.start()
    for read, write in zip(reads, writes):
        read.wait()
        write.start()
    for copy in writes:
        copy.wait()


def outputs(arrays):
    hbm = pl.BlockSpec(memory_space=pl.ANY)
    return pl.pallas_call(
        put_out,
        out_shape=tuple(jax.ShapeDtypeStruct(a.shape, a.dtype) for a in arrays),
        in_specs=[hbm] * len(arrays),
        out_specs=tuple([hbm] * len(arrays)),
        scratch_shapes=[pltpu.VMEM(a.shape, a.dtype) for a in arrays]
        + [pltpu.SemaphoreType.DMA((2, len(arrays)))],
        compiler_params=pltpu.CompilerParams(vmem_limit_bytes=67043328),
        name="outputs",
    )(*arrays)


def shards(tokens, norm_gain, gate_weight, up_weight, down_weight, routes, route_weights):
    sizes = (lax.axis_size("fs_0"), lax.axis_size("tp"), lax.axis_size("grp"))
    gate_serve, up_serve, down_serve, mixture = outputs(
        exchange_and_apply(
            tokens, routes.T, route_weights.T, norm_gain[None, :], gate_weight, up_weight, down_weight, sizes
        )
    )
    return (
        gate_serve.reshape(1, -1, gate_serve.shape[2]),
        up_serve.reshape(1, -1, up_serve.shape[2]),
        down_serve.reshape(1, -1, down_serve.shape[2]),
        mixture,
    )


def solution(mesh):
    split = Mesh(
        mesh.devices.reshape(mesh.shape["grp"], mesh.shape["fs"] // 2, 2, mesh.shape["tp"]),
        ("grp", "fs_0", "fs_1", "tp"),
    )
    placed = (
        P(GRP_FS, "tp"),
        P(FS),
        P(None, FS, "tp"),
        P(None, FS, "tp"),
        P(None, FS, "tp"),
        P(GRP_FS, None),
        P(GRP_FS, None),
    )
    return jax.shard_map(
        shards,
        mesh=split,
        in_specs=placed,
        out_specs=(
            P(GRP_FS, None, "tp"),
            P(GRP_FS, None, "tp"),
            P(GRP_FS, None, "tp"),
            P(GRP_FS, "tp"),
        ),
        check_vma=False,
    )
```
